128 devices in a mesh: fs: 16 (over z, y), tp: 8 (over x, core).
Axes of the slice: x: 4, y: 4, z: 4, core: 2. Of those that a mesh axis runs over, the one named last changes fastest.
Arguments:
- tokens: bfloat16 [8192, 4096], P('fs'), may hold values from -6 to 6
- norm_gain: float32 [4096], P('fs'), may hold values from 0.1 to 1.9
- gate_train: float32 [16, 4096, 1024], P(None, 'fs', 'tp'), may hold values from -0.09375 to 0.09375
- up_train: float32 [16, 4096, 1024], P(None, 'fs', 'tp'), may hold values from -0.09375 to 0.09375
- down_train: float32 [16, 1024, 4096], P(None, 'fs', 'tp'), may hold values from -0.1875 to 0.1875
- shared_gate_train: float32 [4096, 1024], P('fs', 'tp'), may hold values from -0.09375 to 0.09375
- shared_up_train: float32 [4096, 1024], P('fs', 'tp'), may hold values from -0.09375 to 0.09375
- shared_down_train: float32 [1024, 4096], P('fs', 'tp'), may hold values from -0.1875 to 0.1875
- route_expert: int32 [8192, 2], P('fs'), may hold values from 0 to 15, all different within a row; in each aligned block of 512 rows (0 to 511, 512 to 1023, ...) at most 96 rows name the same one
- route_weight: float32 [8192, 2], P('fs'), may hold values from 0.1 to 1
Outputs:
- expert_gate: bfloat16 [16, 4096, 1024], P('fs', None, 'tp')
- expert_up: bfloat16 [16, 4096, 1024], P('fs', None, 'tp')
- expert_down: bfloat16 [16, 1024, 4096], P('fs', 'tp')
- shared_gate: bfloat16 [4096, 1024], P(None, 'tp')
- shared_up: bfloat16 [4096, 1024], P(None, 'tp')
- shared_down: bfloat16 [1024, 4096], P('tp')
- mixed: bfloat16 [8192, 4096], P('fs', 'tp')
The draws below stay inside these ranges and needn't reach their ends.
Inputs may be any that keep to these rules, and one draw needn't show every extreme that they name: `route_expert`: each row names 2 different experts. Within each aligned block of 512 rows no expert is named by more than 96 rows, a bound that some block reaches in every draw.
All inputs are finite; a program needn't handle non-finite values.
Results may differ from the reference program's by a relative error of at most 0.015.
Values may be sent and summed in bfloat16 or wider, within the bound.
A program may use at most 128 MiB of HBM per device.

```python
import math
import jax
import jax.numpy as jnp
import numpy as np
from jax import lax

D = 4096
H = 1024
HS = 1024
TOPK = 2
TOK_DEV = 512
EXPERTS = 16
CAP = 96
TOKENS = 8192
N_FS = 16
N_TP = 8


def levels(rng, dims, shards, low, top_value):
    loudness = 1.0
    for axis_at, shards_of in shards:
        draws = jax.random.uniform(jax.random.fold_in(jax.random.fold_in(rng, 6), axis_at), (shards_of,), jnp.float32, low / len(shards), top_value / len(shards))
        loudness = loudness * jnp.repeat(jnp.exp(draws), dims[axis_at] // shards_of).reshape((-1,) + (1,) * (len(dims) - 1 - axis_at))
    return loudness


def shared_out(key, own, number, rows, amount, top, reach, lean):
    sequence = jax.random.permutation(key, amount)
    crowded, ordinary = shares(amount, rows * top, reach, lean, True), shares(amount, rows * top, reach, lean, False)
    places = jnp.arange(amount)

    def named(sizes, rotation):
        used = int((sizes > 0).sum())
        fixed = max(1, used // 4)
        shifted = fixed + (places - fixed + rotation * (used - fixed)) % max(1, amount - fixed)
        return jnp.zeros((amount,), jnp.int32).at[sequence[jnp.where(places < fixed, places, shifted)]].set(jnp.asarray(sizes, jnp.int32))

    sizes = jnp.where(number % 4 == 0, named(crowded, number // 4), named(ordinary, number - number // 4 - 1))
    mixed = jax.random.permutation(jax.random.fold_in(own, 3), amount)
    giver, taker = mixed[0:amount // 2 * 2:2], mixed[1:amount // 2 * 2:2]
    margin = jnp.minimum(sizes[giver] - 1, reach - sizes[taker]) // 2
    margin = jnp.where((giver == sequence[0]) | (taker == sequence[0]) | (sizes[taker] == 0), 0, jnp.maximum(margin, 0))
    shifted = jax.random.randint(jax.random.fold_in(own, 4), (amount // 2,), 0, 1 << 20) % (margin + 1)
    sizes = sizes.at[giver].add(-shifted).at[taker].add(shifted)
    labels = jnp.searchsorted(jnp.cumsum(sizes), jnp.arange(rows * top), side="right").astype(jnp.int32)
    table = labels.reshape(top, rows).T
    table = table[jax.random.permutation(jax.random.fold_in(own, 1), rows)]
    rotation = jax.random.randint(jax.random.fold_in(own, 2), (rows, 1), 0, top)
    return jnp.take_along_axis(table, (jnp.arange(top)[None, :] + rotation) % top, axis=1)


def shares(amount, total, reach, skew, full):
    portions = [(1 << 20) // math.isqrt(standing ** skew) + 1 for standing in range(1, amount + 1)]
    largest = reach if full else min(reach, max(-(-total // amount), total * portions[0] // sum(portions)))
    least = 1 if total - largest >= amount - 1 else 0
    holding, surplus = [largest] + [least] * (amount - 1), total - largest - least * (amount - 1)
    while surplus > 0:
        free = [i for i in range(1, amount) if holding[i] < largest] or [i for i in range(1, amount) if holding[i] < reach]
        whole, left = sum([portions[i] for i in free]), surplus
        for i in free:
            more = min(reach - holding[i], max(1, left * portions[i] // whole), surplus)
            holding[i] = holding[i] + more
            surplus = surplus - more
    return np.array(holding)


def noise(own_key, extent, spread, limit, shards=(), kind=jnp.bfloat16):
    loudness = levels(own_key, extent, shards, -0.22, 0.18) if shards else 1.0
    array = jax.random.normal(own_key, extent, jnp.float32) * spread * loudness
    return jnp.minimum(jnp.maximum(array, -limit), limit).astype(kind)


def setup_inputs(seed: int = 0) -> dict:
    keys = jax.random.split(jax.random.key(seed), 11)
    tokens = noise(keys[0], (TOKENS, D), 1.0, 6.0, ((0, 16),))
    norm_gain = jnp.clip(1.0 + 0.18 * jax.random.normal(keys[1], (D,), jnp.float32), 0.1, 1.9)
    gate_train = noise(keys[2], (EXPERTS, D, H), D ** -0.5, 0.09375, ((1, 16), (2, 8)), jnp.float32)
    up_train = noise(keys[3], (EXPERTS, D, H), D ** -0.5, 0.09375, ((1, 16), (2, 8)), jnp.float32)
    down_train = noise(keys[4], (EXPERTS, H, D), H ** -0.5, 0.1875, ((1, 16), (2, 8)), jnp.float32)
    shared_gate_train = noise(keys[5], (D, HS), D ** -0.5, 0.09375, ((0, 16), (1, 8)), jnp.float32)
    shared_up_train = noise(keys[6], (D, HS), D ** -0.5, 0.09375, ((0, 16), (1, 8)), jnp.float32)
    shared_down_train = noise(keys[7], (HS, D), HS ** -0.5, 0.1875, ((0, 16), (1, 8)), jnp.float32)
    route_expert_keys = jax.random.split(jax.random.fold_in(keys[8], 1), TOKENS // TOK_DEV)
    route_expert_turns = jax.random.permutation(jax.random.fold_in(keys[8], 3), TOKENS // TOK_DEV)
    route_expert = jax.vmap(lambda own, number: shared_out(jax.random.fold_in(keys[8], 2), own, number, TOK_DEV, EXPERTS, TOPK, CAP, 1))(route_expert_keys, route_expert_turns).reshape((TOKENS, TOPK))
    route_weight = jnp.clip(jnp.exp(math.log(1.0) - 2.3025851 * jax.random.uniform(keys[9], (TOKENS, TOPK), jnp.float32) ** levels(keys[9], (TOKENS, TOPK), ((0, 16),), -0.2, 0.2)), 0.1, 1.0)
    return {"tokens": tokens, "norm_gain": norm_gain, "gate_train": gate_train, "up_train": up_train, "down_train": down_train, "shared_gate_train": shared_gate_train, "shared_up_train": shared_up_train, "shared_down_train": shared_down_train, "route_expert": route_expert, "route_weight": route_weight}


norm_eps = 1e-06

def expert_apply(rows, weight_gate, weight_up, weight_down, pieces):
    gate_vals = jnp.dot(rows, weight_gate, preferred_element_type=jnp.float32)
    up_vals = jnp.dot(rows, weight_up, preferred_element_type=jnp.float32)
    hidden = (jax.nn.silu(gate_vals) * up_vals).astype(jnp.bfloat16)
    step_width = hidden.shape[1] // pieces
    total = jnp.zeros((rows.shape[0], weight_down.shape[1]), jnp.float32)
    for block in range(pieces):
        term = jnp.dot(hidden[:, block * step_width:(block + 1) * step_width], weight_down[block * step_width:(block + 1) * step_width], preferred_element_type=jnp.float32)
        total = total + term.astype(jnp.bfloat16).astype(jnp.float32)
    return total

def reference(tokens, norm_gain, gate_train, up_train, down_train, shared_gate_train, shared_up_train, shared_down_train, route_expert, route_weight):
    expert_gate = (norm_gain[None, :, None] * gate_train).astype(jnp.bfloat16)
    expert_up = (norm_gain[None, :, None] * up_train).astype(jnp.bfloat16)
    expert_down = down_train.astype(jnp.bfloat16)
    shared_gate = (norm_gain[:, None] * shared_gate_train).astype(jnp.bfloat16)
    shared_up = (norm_gain[:, None] * shared_up_train).astype(jnp.bfloat16)
    shared_down = shared_down_train.astype(jnp.bfloat16)
    values = tokens.astype(jnp.float32)
    normed = (values * lax.rsqrt(lax.optimization_barrier(jnp.mean(values * values, axis=1, keepdims=True)) + norm_eps)).astype(jnp.bfloat16)
    pairs = route_expert.reshape(N_FS, TOK_DEV * TOPK)
    chosen = (pairs[:, :, None] == jnp.arange(EXPERTS, dtype=jnp.int32)[None, None, :]).astype(jnp.int32)
    earlier = (jnp.cumsum(chosen, axis=1) - chosen).astype(jnp.int32)
    slot = lax.optimization_barrier(jnp.sum(earlier * chosen, axis=2)).astype(jnp.int32)
    place = (jnp.arange(N_FS, dtype=jnp.int32)[:, None] * CAP + slot).reshape(-1).astype(jnp.int32)
    expert_flat = route_expert.reshape(-1).astype(jnp.int32)
    token_of = (jnp.arange(TOKENS * TOPK, dtype=jnp.int32) // TOPK).astype(jnp.int32)
    table = jnp.zeros((EXPERTS, N_FS * CAP), jnp.int32).at[expert_flat, place].set(token_of)

    def one_expert(operands):
        row_index, weight_gate, weight_up, weight_down = operands
        rows = normed[row_index]
        return expert_apply(rows, weight_gate, weight_up, weight_down, N_TP).astype(jnp.bfloat16)
    results = lax.map(one_expert, (table, expert_gate, expert_up, expert_down))
    picked = results[expert_flat, place].reshape(TOKENS, TOPK, D)
    routed = lax.optimization_barrier(jnp.sum(route_weight[:, :, None] * picked.astype(jnp.float32), axis=1))
    shared_result = expert_apply(normed, shared_gate, shared_up, shared_down, N_TP)
    mixed = (routed + shared_result).astype(jnp.bfloat16)
    return (expert_gate, expert_up, expert_down, shared_gate, shared_up, shared_down, mixed)
```

```python
import jax
import jax.numpy as jnp
from jax import lax
from jax.experimental import pallas as pl
from jax.experimental.pallas import tpu as pltpu
from jax.sharding import PartitionSpec as P

norm_eps = 1e-06
MESH = pl.DeviceIdType.MESH
F32 = jnp.float32
BF16 = jnp.bfloat16
CAP = 96
GROUP = 4 * CAP
HALF = GROUP // 2
TOK = 512
D = 4096
COL = 512
H = 1024
HB = 128
ROWS = 16 * CAP
ORDER = (0, 1, 3, 2)
NEAR = [(a, b) for a in ORDER for b in ORDER if (a, b) != (0, 0)]
FAR = NEAR[::-1]


def dot(a, b):
    return jnp.dot(a, b, preferred_element_type=F32)


def kernel(
    tok_in,
    gain_in,
    gate_in,
    up_in,
    dn_in,
    shg_in,
    shu_in,
    shd_in,
    route,
    weight,
    eg_out,
    eu_out,
    ed_out,
    sg_out,
    su_out,
    sd_out,
    mix_out,
    tok,
    gate_f,
    up_f,
    dn_f,
    shg_f,
    shu_f,
    shd_f,
    gain_col,
    scale_col,
    own,
    outgoing,
    arrived,
    gu_send,
    gu,
    dn_send,
    dcol,
    drow,
    shgu,
    sdcol,
    sdrow,
    acc,
    hid,
    rsend,
    ret,
    comb,
    macc,
    mixv,
    ss,
    rs,
    ls,
    os,
):
    f = lax.axis_index("fs")
    c = lax.axis_index("tp")
    z, y = f // 4, f % 4
    x, k = c // 2, c % 2

    def fs_of(oz, oy):
        return ((z + oz) % 4) * 4 + (y + oy) % 4

    def tp_of(d, other=0):
        return ((x + d) % 4) * 2 + (k + other) % 2

    def fs_dev(oz, oy):
        return (fs_of(oz, oy), c)

    def tp_dev(d, other=0):
        return (f, tp_of(d, other))

    partner = tp_dev(0, 1)
    sent = []
    keys = {}

    def place(key):
        return keys.setdefault(key, len(keys))

    def send(src, dst, key, dev):
        copy = pltpu.make_async_remote_copy(
            src_ref=src,
            dst_ref=dst,
            send_sem=ss.at[len(sent)],
            recv_sem=rs.at[place(key)],
            device_id=dev,
            device_id_type=MESH,
        )
        copy.start()
        sent.append(copy)

    def arrive(dst, key):
        pltpu.make_async_remote_copy(
            src_ref=dst,
            dst_ref=dst,
            send_sem=ss.at[0],
            recv_sem=rs.at[place(key)],
            device_id=partner,
            device_id_type=MESH,
        ).wait_recv()

    def cols(tp_index, width):
        return pl.ds(pl.multiple_of(tp_index * width, width), width)

    def block(index, width):
        return pl.ds(pl.multiple_of(index * width, width), width)

    loads = {}
    for n, (name, src, dst) in enumerate(
        (
            ("tok", tok_in, tok),
            ("gate", gate_in, gate_f),
            ("up", up_in, up_f),
            ("shg", shg_in, shg_f),
            ("shu", shu_in, shu_f),
            ("dn", dn_in, dn_f),
            ("shd", shd_in, shd_f),
        )
    ):
        loads[name] = pltpu.make_async_copy(src, dst, ls.at[n])
        loads[name].start()

    barrier = pltpu.get_barrier_semaphore()
    for oz, oy in NEAR:
        pl.semaphore_signal(barrier, inc=1, device_id=fs_dev(oz, oy), device_id_type=MESH)
    for d in range(4):
        for other in range(2):
            if (d, other) != (0, 0):
                pl.semaphore_signal(
                    barrier, inc=1, device_id=tp_dev(d, other), device_id_type=MESH
                )

    r0, r1 = route[0:1, :], route[1:2, :]
    e_row = lax.broadcasted_iota(jnp.int32, (16, TOK), 0)
    is0, is1 = e_row == r0, e_row == r1
    named = jnp.where(is0 | is1, 1.0, 0.0).astype(BF16)
    before = jnp.where(
        lax.broadcasted_iota(jnp.int32, (TOK, TOK), 0)
        < lax.broadcasted_iota(jnp.int32, (TOK, TOK), 1),
        1.0,
        0.0,
    ).astype(BF16)
    earlier = dot(named, before)

    def target_of(r, hit):
        slot = jnp.sum(jnp.where(hit, earlier, 0.0), axis=0, keepdims=True)
        relative = (((r // 4) - z + 4) % 4) * 4 + ((r % 4) - y + 4) % 4
        return relative.astype(F32) * float(CAP) + slot

    t0, t1 = target_of(r0, is0), target_of(r1, is1)

    diag = lax.broadcasted_iota(jnp.int32, (256, 256), 0) == lax.broadcasted_iota(
        jnp.int32, (256, 256), 1
    )
    gain_col[...] = jnp.broadcast_to(
        jnp.sum(jnp.where(diag, gain_in[...], 0.0), axis=1, keepdims=True), (256, HB)
    )

    loads["tok"].wait()

    def scale_step(i, carry):
        rows = pl.ds(pl.multiple_of(i * 16, 16), 16)
        v = tok[rows, :].astype(F32)
        s = lax.rsqrt(jnp.sum(v * v, axis=1, keepdims=True) * (1.0 / D) + norm_eps)
        scale_col[rows, :] = jnp.broadcast_to(s, (16, HB))
        mine = tok[rows, cols(c, COL)].astype(F32)
        own[rows, :] = (mine * s).astype(BF16)
        return carry

    lax.fori_loop(0, TOK // 16, scale_step, 0)

    for n, g in enumerate(ORDER):
        s_row = (lax.broadcasted_iota(jnp.int32, (GROUP, TOK), 0) + g * GROUP).astype(F32)
        placing = jnp.where((s_row == t0) | (s_row == t1), 1.0, 0.0).astype(BF16)
        outgoing[g * GROUP : (g + 1) * GROUP, :] = dot(placing, own[...]).astype(BF16)
        if n == 0:
            pl.semaphore_wait(barrier, 22)
        for dy in ORDER:
            if (g, dy) != (0, 0):
                there = ((4 - g) % 4) * 4 + (4 - dy) % 4
                send(
                    outgoing.at[pl.ds((g * 4 + dy) * CAP, CAP)],
                    arrived.at[pl.ds(there * CAP, CAP), cols(c, COL)],
                    ("tok", there),
                    fs_dev(g, dy),
                )
    arrived[0:CAP, cols(c, COL)] = outgoing[0:CAP, :]

    loads["gate"].wait()
    loads["up"].wait()

    def gu_step(e, carry):
        gu_send[e, :, 0:HB] = (gate_f[e] * gain_col[...]).astype(BF16)
        gu_send[e, :, HB : 2 * HB] = (up_f[e] * gain_col[...]).astype(BF16)
        return carry

    lax.fori_loop(0, 16, gu_step, 0)
    for part in range(2):
        for oz, oy in FAR:
            there = ((4 - oz) % 4) * 4 + (4 - oy) % 4
            send(
                gu_send.at[fs_of(oz, oy), pl.ds(part * 128, 128)],
                gu.at[pl.ds(pl.multiple_of(f * 256 + part * 128, 128), 128)],
                ("gu", part, there),
                fs_dev(oz, oy),
            )
    gu[block(f, 256), :] = gu_send[f]

    def token_first(g):
        for dy in ORDER:
            if (g, dy) != (0, 0):
                s = g * 4 + dy
                arrive(arrived.at[pl.ds(s * CAP, CAP), cols(c, COL)], ("tok", s))
        piece = arrived.at[pl.ds(g * GROUP, GROUP), cols(c, COL)]
        send(piece, piece, ("xm", g), tp_dev(1))
        send(piece, piece, ("xp", g), tp_dev(3))
        send(piece, piece, ("kp", g, 0), partner)

    def token_second(g):
        for name, d, then, on, start in (("xm", 3, "ft", 1, 0), ("xp", 1, "fb", 3, HALF)):
            piece = arrived.at[pl.ds(g * GROUP, GROUP), cols(tp_of(d), COL)]
            arrive(piece, (name, g))
            part = arrived.at[pl.ds(g * GROUP + start, HALF), cols(tp_of(d), COL)]
            send(part, part, (then, g), tp_dev(on))
            send(piece, piece, ("kp", g, d), partner)

    def token_third(g):
        for name, start in (("ft", 0), ("fb", HALF)):
            part = arrived.at[pl.ds(g * GROUP + start, HALF), cols(tp_of(2), COL)]
            arrive(part, (name, g))
        piece = arrived.at[pl.ds(g * GROUP, GROUP), cols(tp_of(2), COL)]
        send(piece, piece, ("kp", g, 2), partner)

    def silu_times(gate, up):
        return (gate / (1.0 + jnp.exp(-gate)) * up).astype(BF16)

    def hidden_out(g, rows):
        piece = hid.at[rows, cols(c, HB)]
        for d in (1, 3, 2):
            send(piece, piece, ("hx", g, 4 - d), tp_dev(d))
        send(piece, piece, ("hk", g, 0), partner)

    def hidden_rows(g):
        return pl.ds(g * GROUP, GROUP) if g < 4 else pl.ds(ROWS, TOK)

    def expert_hidden(g):
        for d in range(4):
            piece = arrived.at[pl.ds(g * GROUP, GROUP), cols(tp_of(d, 1), COL)]
            arrive(piece, ("kp", g, d))
        rows = pl.ds(g * GROUP, GROUP)
        acc[0:GROUP] = jnp.zeros((GROUP, 2 * HB), F32)

        def step(i, carry):
            acc[0:GROUP] += dot(arrived[rows, block(i, COL)], gu[block(i, COL), :])
            return carry

        lax.fori_loop(0, 8, step, 0)
        hid[rows, cols(c, HB)] = silu_times(acc[0:GROUP, 0:HB], acc[0:GROUP, HB:])
        hidden_out(g, rows)

    def hidden_second(g):
        rows = hidden_rows(g)
        for d in (1, 3, 2):
            piece = hid.at[rows, cols(tp_of(d), HB)]
            arrive(piece, ("hx", g, d))
            send(piece, piece, ("hk", g, d), partner)

    def hidden_last(g):
        rows = hidden_rows(g)
        for d in range(4):
            arrive(hid.at[rows, cols(tp_of(d, 1), HB)], ("hk", g, d))

    def expert_down(g):
        hidden_last(g)
        rows = pl.ds(g * GROUP, GROUP)
        rsend[rows, :] = dot(hid[rows, :], dcol[...]).astype(BF16)
        for dy in ORDER:
            if (g, dy) != (0, 0):
                there = ((4 - g) % 4) * 4 + (4 - dy) % 4
                send(
                    rsend.at[pl.ds((g * 4 + dy) * CAP, CAP)],
                    ret.at[pl.ds(there * CAP, CAP)],
                    ("ret", there),
                    fs_dev(g, dy),
                )
        if g == 0:
            ret[0:CAP, :] = rsend[0:CAP, :]

    def line(j, d):
        return fs_of(k * j + (1 - k) * d, (1 - k) * j + k * d)

    def spread_first(name, ref, height):
        piece = ref.at[block(f, height)]
        for d in (1, 3, 2):
            send(piece, piece, (name, 4 - d), (line(d, 0), c))

    def spread_second(name, ref, height):
        for j in (0, 1, 3, 2):
            piece = ref.at[block(line(j, 0), height)]
            if j:
                arrive(piece, (name, j))
            for d in (1, 3, 2):
                send(piece, piece, (name, j, 4 - d), (line(0, d), c))

    def spread_last(name, ref, height):
        for j in range(4):
            for d in (1, 2, 3):
                arrive(ref.at[block(line(j, d), height)], (name, j, d))

    def across(name, src, dst):
        for d in (1, 3, 2, 0):
            for other in range(2):
                if (d, other) != (0, 0):
                    send(
                        src.at[cols(tp_of(d, other), HB)],
                        dst.at[:, cols(c, COL)],
                        (name, (4 - d) % 4, other),
                        tp_dev(d, other),
                    )
        dst[:, cols(c, COL)] = src[cols(c, HB), :]

    def across_last(name, dst):
        for d in range(4):
            for other in range(2):
                if (d, other) != (0, 0):
                    arrive(dst.at[:, cols(tp_of(d, other), COL)], (name, d, other))

    writes = []

    def write(src, dst):
        copy = pltpu.make_async_copy(src, dst, os.at[len(writes)])
        copy.start()
        writes.append(copy)

    loads["shg"].wait()
    loads["shu"].wait()
    shgu[block(f, 256), 0:HB] = (shg_f[...] * gain_col[...]).astype(BF16)
    shgu[block(f, 256), HB : 2 * HB] = (shu_f[...] * gain_col[...]).astype(BF16)
    token_first(0)
    spread_first("sh", shgu, 256)

    loads["dn"].wait()

    def dn_step(e, carry):
        dn_send[e] = dn_f[e].astype(BF16)
        return carry

    lax.fori_loop(0, 16, dn_step, 0)
    for oz, oy in FAR:
        there = ((4 - oz) % 4) * 4 + (4 - oy) % 4
        send(dn_send.at[fs_of(oz, oy)], dcol.at[block(f, 64)], ("dn", there), fs_dev(oz, oy))
    dcol[block(f, 64), :] = dn_send[f]
    loads["shd"].wait()
    sdcol[block(f, 64), :] = shd_f[...].astype(BF16)
    spread_first("sd", sdcol, 64)

    def norm_step(i, carry):
        rows = pl.ds(pl.multiple_of(i * 16, 16), 16)
        tok[rows, :] = (tok[rows, :].astype(F32) * scale_col[rows, 0:1]).astype(BF16)
        return carry

    lax.fori_loop(0, TOK // 16, norm_step, 0)

    token_first(1)
    token_second(0)
    token_first(3)
    token_second(1)
    token_third(0)
    token_first(2)

    packed = jnp.concatenate([t0, t1, weight[...], jnp.zeros((4, TOK), F32)], axis=0)
    by_token = packed.T
    for g in range(4):
        s_col = (lax.broadcasted_iota(jnp.int32, (TOK, GROUP), 1) + g * GROUP).astype(F32)
        comb[:, g * GROUP : (g + 1) * GROUP] = (
            jnp.where(s_col == by_token[:, 0:1], by_token[:, 2:3], 0.0)
            + jnp.where(s_col == by_token[:, 1:2], by_token[:, 3:4], 0.0)
        ).astype(BF16)

    token_second(3)
    token_third(1)
    spread_second("sh", shgu, 256)
    spread_second("sd", sdcol, 64)
    for part in range(2):
        for oz, oy in NEAR:
            arrive(
                gu.at[pl.ds(pl.multiple_of(fs_of(oz, oy) * 256 + part * 128, 128), 128)],
                ("gu", part, oz * 4 + oy),
            )
    write(gu.at[:, pl.ds(0, HB)], eg_out.at[0])
    write(gu.at[:, pl.ds(HB, HB)], eu_out.at[0])
    expert_hidden(0)
    token_second(2)
    token_third(3)
    expert_hidden(1)
    hidden_second(0)
    token_third(2)
    expert_hidden(3)
    hidden_second(1)

    spread_last("sh", shgu, 256)
    write(shgu.at[:, pl.ds(0, HB)], sg_out)
    write(shgu.at[:, pl.ds(HB, HB)], su_out)
    acc[...] = jnp.zeros((TOK, 2 * HB), F32)

    def shared_step(i, carry):
        acc[...] += dot(tok[:, block(i, COL)], shgu[block(i, COL), :])
        return carry

    lax.fori_loop(0, 8, shared_step, 0)
    hid[ROWS : ROWS + TOK, cols(c, HB)] = silu_times(acc[:, 0:HB], acc[:, HB:])
    expert_hidden(2)
    hidden_out(4, hidden_rows(4))
    hidden_second(3)
    for oz, oy in NEAR:
        arrive(dcol.at[block(fs_of(oz, oy), 64)], ("dn", oz * 4 + oy))
    expert_down(0)
    across("dx", dcol, drow)
    expert_down(1)
    hidden_second(2)
    expert_down(3)
    hidden_second(4)
    expert_down(2)

    spread_last("sd", sdcol, 64)
    across("sx", sdcol, sdrow)
    hidden_last(4)
    macc[...] = dot(hid[ROWS : ROWS + TOK, :], sdcol[...])
    for g in ORDER:
        oz = (4 - g) % 4
        for oy in ORDER:
            if (oz, oy) != (0, 0):
                s = oz * 4 + oy
                arrive(ret.at[pl.ds(s * CAP, CAP)], ("ret", s))
        macc[...] += dot(comb[:, oz * GROUP : (oz + 1) * GROUP], ret[oz * GROUP : (oz + 1) * GROUP])
    mixv[...] = macc[...].astype(BF16)
    write(mixv, mix_out)
    across_last("dx", drow)
    write(drow, ed_out.at[0])
    across_last("sx", sdrow)
    write(sdrow, sd_out)
    for copy in sent:
        copy.wait_send()
    for copy in writes:
        copy.wait()


def on_device(
    tokens,
    norm_gain,
    gate_train,
    up_train,
    down_train,
    shared_gate_train,
    shared_up_train,
    shared_down_train,
    route_expert,
    route_weight,
):
    hbm = pl.BlockSpec(memory_space=pl.ANY)
    vmem = pl.BlockSpec(memory_space=pltpu.VMEM)
    return pl.pallas_call(
        kernel,
        out_shape=(
            jax.ShapeDtypeStruct((1, D, HB), BF16),
            jax.ShapeDtypeStruct((1, D, HB), BF16),
            jax.ShapeDtypeStruct((1, HB, D), BF16),
            jax.ShapeDtypeStruct((D, HB), BF16),
            jax.ShapeDtypeStruct((D, HB), BF16),
            jax.ShapeDtypeStruct((HB, D), BF16),
            jax.ShapeDtypeStruct((TOK, COL), BF16),
        ),
        in_specs=[hbm, vmem, hbm, hbm, hbm, hbm, hbm, hbm, vmem, vmem],
        out_specs=(hbm,) * 7,
        scratch_shapes=[
            pltpu.VMEM((TOK, D), BF16),
            pltpu.VMEM((16, 256, HB), F32),
            pltpu.VMEM((16, 256, HB), F32),
            pltpu.VMEM((16, 64, COL), F32),
            pltpu.VMEM((256, HB), F32),
            pltpu.VMEM((256, HB), F32),
            pltpu.VMEM((64, COL), F32),
            pltpu.VMEM((256, HB), F32),
            pltpu.VMEM((TOK, HB), F32),
            pltpu.VMEM((TOK, COL), BF16),
            pltpu.VMEM((ROWS, COL), BF16),
            pltpu.VMEM((ROWS, D), BF16),
            pltpu.VMEM((16, 256, 2 * HB), BF16),
            pltpu.VMEM((D, 2 * HB), BF16),
            pltpu.VMEM((16, 64, COL), BF16),
            pltpu.VMEM((H, COL), BF16),
            pltpu.VMEM((HB, D), BF16),
            pltpu.VMEM((D, 2 * HB), BF16),
            pltpu.VMEM((H, COL), BF16),
            pltpu.VMEM((HB, D), BF16),
            pltpu.VMEM((TOK, 2 * HB), F32),
            pltpu.VMEM((ROWS + TOK, H), BF16),
            pltpu.VMEM((ROWS, COL), BF16),
            pltpu.VMEM((ROWS, COL), BF16),
            pltpu.VMEM((TOK, ROWS), BF16),
            pltpu.VMEM((TOK, COL), F32),
            pltpu.VMEM((TOK, COL), BF16),
            pltpu.SemaphoreType.DMA((192,)),
            pltpu.SemaphoreType.DMA((192,)),
            pltpu.SemaphoreType.DMA((7,)),
            pltpu.SemaphoreType.DMA((7,)),
        ],
        compiler_params=pltpu.CompilerParams(
            collective_id=0, has_side_effects=True, vmem_limit_bytes=62 * 1024 * 1024
        ),
        name="layer",
    )(
        tokens,
        norm_gain.reshape(1, 256),
        gate_train,
        up_train,
        down_train,
        shared_gate_train,
        shared_up_train,
        shared_down_train,
        route_expert.T,
        route_weight.T,
    )


def solution(mesh):
    placed = (
        P("fs", None),
        P("fs"),
        P(None, "fs", "tp"),
        P(None, "fs", "tp"),
        P(None, "fs", "tp"),
        P("fs", "tp"),
        P("fs", "tp"),
        P("fs", "tp"),
        P("fs", None),
        P("fs", None),
    )
    return jax.shard_map(
        on_device,
        mesh=mesh,
        in_specs=placed,
        out_specs=(
            P("fs", None, "tp"),
            P("fs", None, "tp"),
            P("fs", "tp", None),
            P(None, "tp"),
            P(None, "tp"),
            P("tp", None),
            P("fs", "tp"),
        ),
        check_vma=False,
    )
```

```python
import jax
import jax.numpy as jnp
from jax import lax
from jax.experimental import pallas as pl
from jax.experimental.pallas import tpu as pltpu
from jax.sharding import PartitionSpec as P

norm_eps = 1e-06
MESH = pl.DeviceIdType.MESH
F32 = jnp.float32
BF16 = jnp.bfloat16
CAP = 96
GROUP = 4 * CAP
HALF = GROUP // 2
TOK = 512
D = 4096
COL = 512
H = 1024
HB = 128
ROWS = 16 * CAP
ORDER = (0, 1, 3, 2)
NEAR = [(a, b) for a in ORDER for b in ORDER if (a, b) != (0, 0)]
FAR = NEAR[::-1]
CHUNKS = ((0, CAP), (CAP, 3 * CAP), (GROUP, GROUP), (3 * GROUP, GROUP), (2 * GROUP, GROUP))

PLAN = (
    "t1:1", "t2:0", "t1:2", "t2:1", "t3:0", "sd2", "t1:3", "t2:2", "t3:1", "comb", "norm",
    "t1:4", "t2:3", "t3:2", "t2:4", "t3:3", "gu", "eh:0", "eh:1", "t3:4", "eh:3", "h2:0",
    "eh:2", "h2:1", "sh", "h3:0", "h2:3", "h3:1", "h2:2", "h2:4", "dn", "dx", "ed:0", "ed:1",
    "h3:3", "h3:2", "ed:3", "h3:4", "ed:2", "sd3", "sx", "sdn", "cb:0", "cb:1", "cb:3", "cb:2",
    "dx3", "sx3",
)


def dot(a, b):
    return jnp.dot(a, b, preferred_element_type=F32)


def kernel(
    tok_in,
    gain_in,
    gate_in,
    up_in,
    dn_in,
    shg_in,
    shu_in,
    shd_in,
    route,
    weight,
    gu,
    drow,
    shgu,
    sdrow,
    mixv,
    tok,
    gate_f,
    up_f,
    dn_f,
    shg_f,
    shu_f,
    shd_f,
    gain_col,
    scale_col,
    own,
    outgoing,
    arrived,
    gu_send,
    dn_send,
    dcol,
    sdcol,
    acc,
    hid,
    rsend,
    ret,
    comb,
    macc,
    ss,
    rs,
    ls,
):
    f = lax.axis_index("fs")
    c = lax.axis_index("tp")
    z, y = f // 4, f % 4
    x, k = c // 2, c % 2

    def fs_of(oz, oy):
        return ((z + oz) % 4) * 4 + (y + oy) % 4

    def tp_of(d, other=0):
        return ((x + d) % 4) * 2 + (k + other) % 2

    def fs_dev(oz, oy):
        return (fs_of(oz, oy), c)

    def tp_dev(d, other=0):
        return (f, tp_of(d, other))

    partner = tp_dev(0, 1)
    sent = []
    keys = {}

    def place(key):
        return keys.setdefault(key, len(keys))

    def send(src, dst, key, dev):
        copy = pltpu.make_async_remote_copy(
            src_ref=src,
            dst_ref=dst,
            send_sem=ss.at[len(sent)],
            recv_sem=rs.at[place(key)],
            device_id=dev,
            device_id_type=MESH,
        )
        copy.start()
        sent.append(copy)

    def arrive(dst, key):
        pltpu.make_async_remote_copy(
            src_ref=dst,
            dst_ref=dst,
            send_sem=ss.at[0],
            recv_sem=rs.at[place(key)],
            device_id=partner,
            device_id_type=MESH,
        ).wait_recv()

    def cols(tp_index, width):
        return pl.ds(pl.multiple_of(tp_index * width, width), width)

    def block(index, width):
        return pl.ds(pl.multiple_of(index * width, width), width)

    def load(n, src, dst):
        copy = pltpu.make_async_copy(src, dst, ls.at[n])
        copy.start()
        return copy

    quarter = TOK // 4
    tok_loads = [
        load(n, tok_in.at[pl.ds(n * quarter, quarter)], tok.at[pl.ds(n * quarter, quarter)])
        for n in range(4)
    ]
    shared_loads = [load(4, shg_in, shg_f), load(5, shu_in, shu_f), load(6, shd_in, shd_f)]

    barrier = pltpu.get_barrier_semaphore()
    for oz, oy in NEAR:
        pl.semaphore_signal(barrier, inc=1, device_id=fs_dev(oz, oy), device_id_type=MESH)
    for d in range(4):
        for other in range(2):
            if (d, other) != (0, 0):
                pl.semaphore_signal(
                    barrier, inc=1, device_id=tp_dev(d, other), device_id_type=MESH
                )

    def line(j, d):
        return fs_of(k * j + (1 - k) * d, (1 - k) * j + k * d)

    def spread_first(name, ref, height):
        piece = ref.at[block(f, height)]
        for d in (2, 1, 3):
            send(piece, piece, (name, 4 - d), (line(d, 0), c))

    def spread_second(name, ref, height):
        for j in (0, 1, 3, 2):
            piece = ref.at[block(line(j, 0), height)]
            if j:
                arrive(piece, (name, j))
            for d in (2, 1, 3):
                send(piece, piece, (name, j, 4 - d), (line(0, d), c))

    def spread_last(name, ref, height):
        for j in range(4):
            for d in (1, 2, 3):
                arrive(ref.at[block(line(j, d), height)], (name, j, d))

    r0, r1 = route[0:1, :], route[1:2, :]
    e_row = lax.broadcasted_iota(jnp.int32, (16, TOK), 0)
    is0, is1 = e_row == r0, e_row == r1
    named = jnp.where(is0 | is1, 1.0, 0.0).astype(BF16)
    before = jnp.where(
        lax.broadcasted_iota(jnp.int32, (TOK, TOK), 0)
        < lax.broadcasted_iota(jnp.int32, (TOK, TOK), 1),
        1.0,
        0.0,
    ).astype(BF16)
    earlier = dot(named, before)

    def target_of(r, hit):
        slot = jnp.sum(jnp.where(hit, earlier, 0.0), axis=0, keepdims=True)
        relative = (((r // 4) - z + 4) % 4) * 4 + ((r % 4) - y + 4) % 4
        return relative.astype(F32) * float(CAP) + slot

    t0, t1 = target_of(r0, is0), target_of(r1, is1)

    diag = lax.broadcasted_iota(jnp.int32, (256, 256), 0) == lax.broadcasted_iota(
        jnp.int32, (256, 256), 1
    )
    gain_col[...] = jnp.broadcast_to(
        jnp.sum(jnp.where(diag, gain_in[...], 0.0), axis=1, keepdims=True), (256, HB)
    )

    def square_step(i, carry):
        rows = pl.ds(pl.multiple_of(i * 16, 16), 16)
        total = jnp.zeros((16, HB), F32)
        for j in range(D // HB):
            v = tok[rows, j * HB : (j + 1) * HB].astype(F32)
            total = total + v * v
        scale_col[rows, :] = total
        return carry

    def own_step(i, carry):
        rows = pl.ds(pl.multiple_of(i * 64, 64), 64)
        s = lax.rsqrt(jnp.sum(scale_col[rows, :], axis=1, keepdims=True) * (1.0 / D) + norm_eps)
        scale_col[rows, :] = jnp.broadcast_to(s, (64, HB))
        own[rows, :] = (tok[rows, cols(c, COL)].astype(F32) * s).astype(BF16)
        return carry

    for n in range(4):
        tok_loads[n].wait()
        with jax.named_scope("square"):
            lax.fori_loop(n * 8, n * 8 + 8, square_step, 0, unroll=2)
    weight_loads = [load(7, gate_in, gate_f), load(8, up_in, up_f), load(9, dn_in, dn_f)]
    for copy in shared_loads:
        copy.wait()
    shgu[block(f, 256), 0:HB] = (shg_f[...] * gain_col[...]).astype(BF16)
    shgu[block(f, 256), HB : 2 * HB] = (shu_f[...] * gain_col[...]).astype(BF16)
    sdcol[block(f, 64), :] = shd_f[...].astype(BF16)
    with jax.named_scope("barrier"):
        pl.semaphore_wait(barrier, 22)
    spread_first("sh", shgu, 256)
    with jax.named_scope("own"):
        lax.fori_loop(0, TOK // 64, own_step, 0)

    def token_first(n):
        start, height = CHUNKS[n]
        for s in range(start // CAP, (start + height) // CAP):
            if s:
                arrive(arrived.at[pl.ds(s * CAP, CAP), cols(c, COL)], ("tok", s))
        piece = arrived.at[pl.ds(start, height), cols(c, COL)]
        send(piece, piece, ("xm", n), tp_dev(1))
        send(piece, piece, ("xp", n), tp_dev(3))
        send(piece, piece, ("kp", n, 0), partner)

    def token_second(n):
        start, height = CHUNKS[n]
        half = height // 2
        for name, d, then, on, skip in (("xm", 3, "ft", 1, 0), ("xp", 1, "fb", 3, half)):
            piece = arrived.at[pl.ds(start, height), cols(tp_of(d), COL)]
            arrive(piece, (name, n))
            part = arrived.at[pl.ds(start + skip, half), cols(tp_of(d), COL)]
            send(part, part, (then, n), tp_dev(on))
            send(piece, piece, ("kp", n, d), partner)

    def token_third(n):
        start, height = CHUNKS[n]
        half = height // 2
        for name, skip in (("ft", 0), ("fb", half)):
            part = arrived.at[pl.ds(start + skip, half), cols(tp_of(2), COL)]
            arrive(part, (name, n))
        piece = arrived.at[pl.ds(start, height), cols(tp_of(2), COL)]
        send(piece, piece, ("kp", n, 2), partner)

    def token_last(n):
        start, height = CHUNKS[n]
        for d in range(4):
            arrive(arrived.at[pl.ds(start, height), cols(tp_of(d, 1), COL)], ("kp", n, d))

    with jax.named_scope("dispatch"):
        for g in ORDER:
            s_row = (lax.broadcasted_iota(jnp.int32, (GROUP, TOK), 0) + g * GROUP).astype(F32)
            placing = jnp.where((s_row == t0) | (s_row == t1), 1.0, 0.0).astype(BF16)
            outgoing[g * GROUP : (g + 1) * GROUP, :] = dot(placing, own[...]).astype(BF16)
            for dy in ORDER:
                if (g, dy) != (0, 0):
                    there = ((4 - g) % 4) * 4 + (4 - dy) % 4
                    send(
                        outgoing.at[pl.ds((g * 4 + dy) * CAP, CAP)],
                        arrived.at[pl.ds(there * CAP, CAP), cols(c, COL)],
                        ("tok", there),
                        fs_dev(g, dy),
                    )
            if g == 0:
                arrived[0:CAP, cols(c, COL)] = outgoing[0:CAP, :]
    token_first(0)
    spread_first("sd", sdcol, 64)

    weight_loads[0].wait()
    weight_loads[1].wait()

    def gu_step(e, carry):
        gu_send[e, :, 0:HB] = (gate_f[e] * gain_col[...]).astype(BF16)
        gu_send[e, :, HB : 2 * HB] = (up_f[e] * gain_col[...]).astype(BF16)
        return carry

    with jax.named_scope("gu_cast"):
        lax.fori_loop(0, 16, gu_step, 0)
    for part in range(2):
        for oz, oy in FAR:
            there = ((4 - oz) % 4) * 4 + (4 - oy) % 4
            send(
                gu_send.at[fs_of(oz, oy), pl.ds(part * 128, 128)],
                gu.at[pl.ds(pl.multiple_of(f * 256 + part * 128, 128), 128)],
                ("gu", part, there),
                fs_dev(oz, oy),
            )
    gu[block(f, 256), :] = gu_send[f]
    with jax.named_scope("spread2_sh"):
        spread_second("sh", shgu, 256)
    weight_loads[2].wait()

    def dn_step(e, carry):
        dn_send[e] = dn_f[e].astype(BF16)
        return carry

    lax.fori_loop(0, 16, dn_step, 0)
    for oz, oy in FAR:
        there = ((4 - oz) % 4) * 4 + (4 - oy) % 4
        send(dn_send.at[fs_of(oz, oy)], dcol.at[block(f, 64)], ("dn", there), fs_dev(oz, oy))
    dcol[block(f, 64), :] = dn_send[f]

    def silu_times(gate, up):
        return (gate / (1.0 + jnp.exp(-gate)) * up).astype(BF16)

    def hidden_rows(g):
        return (g * GROUP, GROUP) if g < 4 else (ROWS, TOK)

    def hidden_first(g):
        start, height = hidden_rows(g)
        piece = hid.at[pl.ds(start, height), cols(c, HB)]
        send(piece, piece, ("hm", g), tp_dev(1))
        send(piece, piece, ("hp", g), tp_dev(3))
        send(piece, piece, ("hk", g, 0), partner)

    def hidden_second(g):
        start, height = hidden_rows(g)
        half = height // 2
        for name, d, then, on, skip in (("hm", 3, "ht", 1, 0), ("hp", 1, "hb", 3, half)):
            piece = hid.at[pl.ds(start, height), cols(tp_of(d), HB)]
            arrive(piece, (name, g))
            part = hid.at[pl.ds(start + skip, half), cols(tp_of(d), HB)]
            send(part, part, (then, g), tp_dev(on))
            send(piece, piece, ("hk", g, d), partner)

    def hidden_third(g):
        start, height = hidden_rows(g)
        half = height // 2
        for name, skip in (("ht", 0), ("hb", half)):
            part = hid.at[pl.ds(start + skip, half), cols(tp_of(2), HB)]
            arrive(part, (name, g))
        piece = hid.at[pl.ds(start, height), cols(tp_of(2), HB)]
        send(piece, piece, ("hk", g, 2), partner)

    def hidden_last(g):
        start, height = hidden_rows(g)
        for d in range(4):
            arrive(hid.at[pl.ds(start, height), cols(tp_of(d, 1), HB)], ("hk", g, d))

    def expert_hidden(g):
        for n in ((0, 1), (2,), (4,), (3,))[g]:
            token_last(n)
        rows = pl.ds(g * GROUP, GROUP)
        acc[0:GROUP] = jnp.zeros((GROUP, 2 * HB), F32)

        def step(i, carry):
            acc[0:GROUP] += dot(arrived[rows, block(i, COL)], gu[block(i, COL), :])
            return carry

        lax.fori_loop(0, 8, step, 0)
        hid[rows, cols(c, HB)] = silu_times(acc[0:GROUP, 0:HB], acc[0:GROUP, HB:])
        hidden_first(g)

    def expert_down(g):
        hidden_last(g)
        rows = pl.ds(g * GROUP, GROUP)
        rsend[rows, :] = dot(hid[rows, :], dcol[...]).astype(BF16)
        for dy in ORDER:
            if (g, dy) != (0, 0):
                there = ((4 - g) % 4) * 4 + (4 - dy) % 4
                send(
                    rsend.at[pl.ds((g * 4 + dy) * CAP, CAP)],
                    ret.at[pl.ds(there * CAP, CAP)],
                    ("ret", there),
                    fs_dev(g, dy),
                )
        if g == 0:
            ret[0:CAP, :] = rsend[0:CAP, :]

    def across(name, src, dst):
        for d in (2, 1, 3, 0):
            for other in range(2):
                if (d, other) != (0, 0):
                    send(
                        src.at[cols(tp_of(d, other), HB)],
                        dst.at[:, cols(c, COL)],
                        (name, (4 - d) % 4, other),
                        tp_dev(d, other),
                    )
        dst[:, cols(c, COL)] = src[cols(c, HB), :]

    def across_last(name, dst):
        for d in range(4):
            for other in range(2):
                if (d, other) != (0, 0):
                    arrive(dst.at[:, cols(tp_of(d, other), COL)], (name, d, other))

    def norm_step(i, carry):
        rows = pl.ds(pl.multiple_of(i * 16, 16), 16)
        tok[rows, :] = (tok[rows, :].astype(F32) * scale_col[rows, 0:1]).astype(BF16)
        return carry

    def combine_weights():
        packed = jnp.concatenate([t0, t1, weight[...], jnp.zeros((4, TOK), F32)], axis=0)
        by_token = packed.T
        for g in range(4):
            s_col = (lax.broadcasted_iota(jnp.int32, (TOK, GROUP), 1) + g * GROUP).astype(F32)
            comb[:, g * GROUP : (g + 1) * GROUP] = (
                jnp.where(s_col == by_token[:, 0:1], by_token[:, 2:3], 0.0)
                + jnp.where(s_col == by_token[:, 1:2], by_token[:, 3:4], 0.0)
            ).astype(BF16)

    def gu_last():
        for part in range(2):
            for oz, oy in NEAR:
                start = pl.multiple_of(fs_of(oz, oy) * 256 + part * 128, 128)
                arrive(gu.at[pl.ds(start, 128)], ("gu", part, oz * 4 + oy))

    def dn_last():
        for oz, oy in NEAR:
            arrive(dcol.at[block(fs_of(oz, oy), 64)], ("dn", oz * 4 + oy))

    def shared_hidden():
        spread_last("sh", shgu, 256)
        acc[...] = jnp.zeros((TOK, 2 * HB), F32)

        def step(i, carry):
            acc[...] += dot(tok[:, block(i, COL)], shgu[block(i, COL), :])
            return carry

        lax.fori_loop(0, 8, step, 0)
        hid[ROWS : ROWS + TOK, cols(c, HB)] = silu_times(acc[:, 0:HB], acc[:, HB:])
        hidden_first(4)

    def shared_down():
        hidden_last(4)
        macc[...] = dot(hid[ROWS : ROWS + TOK, :], sdcol[...])

    def combine(g):
        oz = (4 - g) % 4
        for oy in ORDER:
            if (oz, oy) != (0, 0):
                s = oz * 4 + oy
                arrive(ret.at[pl.ds(s * CAP, CAP)], ("ret", s))
        macc[...] += dot(comb[:, oz * GROUP : (oz + 1) * GROUP], ret[oz * GROUP : (oz + 1) * GROUP])

    steps = dict(
        t1=token_first,
        t2=token_second,
        t3=token_third,
        eh=expert_hidden,
        h2=hidden_second,
        h3=hidden_third,
        ed=expert_down,
        cb=combine,
    )
    singles = dict(
        norm=lambda: lax.fori_loop(0, TOK // 16, norm_step, 0, unroll=2),
        comb=combine_weights,
        gu=gu_last,
        dn=dn_last,
        sd2=lambda: spread_second("sd", sdcol, 64),
        sd3=lambda: spread_last("sd", sdcol, 64),
        sh=shared_hidden,
        sdn=shared_down,
        dx=lambda: across("dx", dcol, drow),
        sx=lambda: across("sx", sdcol, sdrow),
        dx3=lambda: across_last("dx", drow),
        sx3=lambda: across_last("sx", sdrow),
    )
    for word in PLAN:
        with jax.named_scope(word.replace(":", "_")):
            if ":" in word:
                name, n = word.split(":")
                steps[name](int(n))
            else:
                singles[word]()
    mixv[...] = macc[...].astype(BF16)
    with jax.named_scope("drain"):
        for copy in sent:
            copy.wait_send()


def writer(gu, drow, shgu, sdrow, mixv, eg, eu, ed, sg, su, sd, mix, sems):
    copies = [
        pltpu.make_async_copy(src, dst, sems.at[n])
        for n, (src, dst) in enumerate(
            (
                (gu.at[:, pl.ds(0, HB)], eg.at[0]),
                (gu.at[:, pl.ds(HB, HB)], eu.at[0]),
                (drow, ed.at[0]),
                (shgu.at[:, pl.ds(0, HB)], sg),
                (shgu.at[:, pl.ds(HB, HB)], su),
                (sdrow, sd),
                (mixv, mix),
            )
        )
    ]
    for copy in copies:
        copy.start()
    for copy in copies:
        copy.wait()


def on_device(
    tokens,
    norm_gain,
    gate_train,
    up_train,
    down_train,
    shared_gate_train,
    shared_up_train,
    shared_down_train,
    route_expert,
    route_weight,
):
    hbm = pl.BlockSpec(memory_space=pl.ANY)
    vmem = pl.BlockSpec(memory_space=pltpu.VMEM)
    kept = pl.pallas_call(
        kernel,
        out_shape=(
            pltpu.VMEM((D, 2 * HB), BF16),
            pltpu.VMEM((HB, D), BF16),
            pltpu.VMEM((D, 2 * HB), BF16),
            pltpu.VMEM((HB, D), BF16),
            pltpu.VMEM((TOK, COL), BF16),
        ),
        in_specs=[hbm, vmem, hbm, hbm, hbm, hbm, hbm, hbm, vmem, vmem],
        out_specs=(vmem,) * 5,
        scratch_shapes=[
            pltpu.VMEM((TOK, D), BF16),
            pltpu.VMEM((16, 256, HB), F32),
            pltpu.VMEM((16, 256, HB), F32),
            pltpu.VMEM((16, 64, COL), F32),
            pltpu.VMEM((256, HB), F32),
            pltpu.VMEM((256, HB), F32),
            pltpu.VMEM((64, COL), F32),
            pltpu.VMEM((256, HB), F32),
            pltpu.VMEM((TOK, HB), F32),
            pltpu.VMEM((TOK, COL), BF16),
            pltpu.VMEM((ROWS, COL), BF16),
            pltpu.VMEM((ROWS, D), BF16),
            pltpu.VMEM((16, 256, 2 * HB), BF16),
            pltpu.VMEM((16, 64, COL), BF16),
            pltpu.VMEM((H, COL), BF16),
            pltpu.VMEM((H, COL), BF16),
            pltpu.VMEM((TOK, 2 * HB), F32),
            pltpu.VMEM((ROWS + TOK, H), BF16),
            pltpu.VMEM((ROWS, COL), BF16),
            pltpu.VMEM((ROWS, COL), BF16),
            pltpu.VMEM((TOK, ROWS), BF16),
            pltpu.VMEM((TOK, COL), F32),
            pltpu.SemaphoreType.DMA((224,)),
            pltpu.SemaphoreType.DMA((224,)),
            pltpu.SemaphoreType.DMA((10,)),
        ],
        compiler_params=pltpu.CompilerParams(
            collective_id=0, has_side_effects=True, vmem_limit_bytes=54 * 1024 * 1024
        ),
        name="layer",
    )(
        tokens,
        norm_gain.reshape(1, 256),
        gate_train,
        up_train,
        down_train,
        shared_gate_train,
        shared_up_train,
        shared_down_train,
        route_expert.T,
        route_weight.T,
    )
    return pl.pallas_call(
        writer,
        out_shape=(
            jax.ShapeDtypeStruct((1, D, HB), BF16),
            jax.ShapeDtypeStruct((1, D, HB), BF16),
            jax.ShapeDtypeStruct((1, HB, D), BF16),
            jax.ShapeDtypeStruct((D, HB), BF16),
            jax.ShapeDtypeStruct((D, HB), BF16),
            jax.ShapeDtypeStruct((HB, D), BF16),
            jax.ShapeDtypeStruct((TOK, COL), BF16),
        ),
        in_specs=[vmem] * 5,
        out_specs=(hbm,) * 7,
        scratch_shapes=[pltpu.SemaphoreType.DMA((7,))],
        compiler_params=pltpu.CompilerParams(vmem_limit_bytes=1024 * 1024),
        name="writer",
    )(*(pltpu.with_memory_space_constraint(a, pltpu.VMEM) for a in kept))


def solution(mesh):
    placed = (
        P("fs", None),
        P("fs"),
        P(None, "fs", "tp"),
        P(None, "fs", "tp"),
        P(None, "fs", "tp"),
        P("fs", "tp"),
        P("fs", "tp"),
        P("fs", "tp"),
        P("fs", None),
        P("fs", None),
    )
    return jax.shard_map(
        on_device,
        mesh=mesh,
        in_specs=placed,
        out_specs=(
            P("fs", None, "tp"),
            P("fs", None, "tp"),
            P("fs", "tp", None),
            P(None, "tp"),
            P(None, "tp"),
            P("tp", None),
            P("fs", "tp"),
        ),
        check_vma=False,
    )
```

```python
import jax
import jax.numpy as jnp
from jax import lax
from jax.experimental import pallas as pl
from jax.experimental.pallas import tpu as pltpu
from jax.sharding import PartitionSpec as P

norm_eps = 1e-06
MESH = pl.DeviceIdType.MESH
F32 = jnp.float32
BF16 = jnp.bfloat16
CAP = 96
GROUP = 4 * CAP
HALF = GROUP // 2
TOK = 512
D = 4096
COL = 512
H = 1024
HB = 128
ROWS = 16 * CAP
ORDER = (0, 1, 3, 2)
NEAR = [(a, b) for a in ORDER for b in ORDER if (a, b) != (0, 0)]
FAR = NEAR[::-1]
CHUNKS = ((0, CAP), (CAP, 3 * CAP), (GROUP, GROUP), (3 * GROUP, GROUP), (2 * GROUP, GROUP))

PLAN = (
    "t1:0", "sd1", "gu1", "gu2", "sh2", "dn1", "t1:1", "t2:0", "comb", "norm", "t1:2", "t2:1",
    "t3:0", "t1:3", "t1:4", "t2:2", "t3:1", "t2:3", "t3:2", "sd2", "t2:4", "t3:3", "gu", "eh:0",
    "eh:1", "t3:4", "eh:3", "h2:0", "eh:2", "h2:1", "sh", "h3:0", "h2:3", "h3:1", "h2:2",
    "h2:4", "dn", "dxa", "dxb", "ed:0", "ed:1", "h3:3", "h3:2", "ed:3", "h3:4", "ed:2", "sd3",
    "sxa", "sxb", "sdn", "cb:0", "cb:1", "cb:3", "cb:2", "dx3", "sx3",
)


def dot(a, b):
    return jnp.dot(a, b, preferred_element_type=F32)


def kernel(
    tok_in,
    gain_in,
    gate_in,
    up_in,
    dn_in,
    shg_in,
    shu_in,
    shd_in,
    route,
    weight,
    gu,
    drow,
    shgu,
    sdrow,
    mixv,
    tok,
    gate_f,
    up_f,
    dn_f,
    shg_f,
    shu_f,
    shd_f,
    gain_col,
    scale_col,
    own,
    outgoing,
    arrived,
    gu_send,
    dn_send,
    dcol,
    sdcol,
    acc,
    hid,
    rsend,
    ret,
    comb,
    macc,
    ss,
    rs,
    ls,
):
    f = lax.axis_index("fs")
    c = lax.axis_index("tp")
    z, y = f // 4, f % 4
    x, k = c // 2, c % 2

    def fs_of(oz, oy):
        return ((z + oz) % 4) * 4 + (y + oy) % 4

    def tp_of(d, other=0):
        return ((x + d) % 4) * 2 + (k + other) % 2

    def fs_dev(oz, oy):
        return (fs_of(oz, oy), c)

    def tp_dev(d, other=0):
        return (f, tp_of(d, other))

    partner = tp_dev(0, 1)
    sent = []
    keys = {}

    def place(key):
        return keys.setdefault(key, len(keys))

    def send(src, dst, key, dev):
        copy = pltpu.make_async_remote_copy(
            src_ref=src,
            dst_ref=dst,
            send_sem=ss.at[len(sent)],
            recv_sem=rs.at[place(key)],
            device_id=dev,
            device_id_type=MESH,
        )
        copy.start()
        sent.append(copy)

    def arrive(dst, key):
        pltpu.make_async_remote_copy(
            src_ref=dst,
            dst_ref=dst,
            send_sem=ss.at[0],
            recv_sem=rs.at[place(key)],
            device_id=partner,
            device_id_type=MESH,
        ).wait_recv()

    def cols(tp_index, width):
        return pl.ds(pl.multiple_of(tp_index * width, width), width)

    def block(index, width):
        return pl.ds(pl.multiple_of(index * width, width), width)

    def load(n, src, dst):
        copy = pltpu.make_async_copy(src, dst, ls.at[n])
        copy.start()
        return copy

    quarter = TOK // 4
    tok_loads = [
        load(n, tok_in.at[pl.ds(n * quarter, quarter)], tok.at[pl.ds(n * quarter, quarter)])
        for n in range(4)
    ]
    shared_loads = [load(4, shg_in, shg_f), load(5, shu_in, shu_f), load(6, shd_in, shd_f)]

    barrier = pltpu.get_barrier_semaphore()
    for oz, oy in NEAR:
        pl.semaphore_signal(barrier, inc=1, device_id=fs_dev(oz, oy), device_id_type=MESH)
    for d in range(4):
        for other in range(2):
            if (d, other) != (0, 0):
                pl.semaphore_signal(
                    barrier, inc=1, device_id=tp_dev(d, other), device_id_type=MESH
                )

    def line(j, d):
        return fs_of(k * j + (1 - k) * d, (1 - k) * j + k * d)

    def spread_first(name, ref, height):
        piece = ref.at[block(f, height)]
        for d in (2, 1, 3):
            send(piece, piece, (name, 4 - d), (line(d, 0), c))

    def spread_second(name, ref, height):
        for j in (0, 1, 3, 2):
            piece = ref.at[block(line(j, 0), height)]
            if j:
                arrive(piece, (name, j))
            for d in (2, 1, 3):
                send(piece, piece, (name, j, 4 - d), (line(0, d), c))

    def spread_last(name, ref, height):
        for j in range(4):
            for d in (1, 2, 3):
                arrive(ref.at[block(line(j, d), height)], (name, j, d))

    r0, r1 = route[0:1, :], route[1:2, :]
    e_row = lax.broadcasted_iota(jnp.int32, (16, TOK), 0)
    is0, is1 = e_row == r0, e_row == r1
    named = jnp.where(is0 | is1, 1.0, 0.0).astype(BF16)
    before = jnp.where(
        lax.broadcasted_iota(jnp.int32, (TOK, TOK), 0)
        < lax.broadcasted_iota(jnp.int32, (TOK, TOK), 1),
        1.0,
        0.0,
    ).astype(BF16)
    earlier = dot(named, before)

    def target_of(r, hit):
        slot = jnp.sum(jnp.where(hit, earlier, 0.0), axis=0, keepdims=True)
        relative = (((r // 4) - z + 4) % 4) * 4 + ((r % 4) - y + 4) % 4
        return relative.astype(F32) * float(CAP) + slot

    t0, t1 = target_of(r0, is0), target_of(r1, is1)

    diag = lax.broadcasted_iota(jnp.int32, (256, 256), 0) == lax.broadcasted_iota(
        jnp.int32, (256, 256), 1
    )
    gain_col[...] = jnp.broadcast_to(
        jnp.sum(jnp.where(diag, gain_in[...], 0.0), axis=1, keepdims=True), (256, HB)
    )

    def square_step(i, carry):
        rows = pl.ds(pl.multiple_of(i * 16, 16), 16)
        total = jnp.zeros((16, HB), F32)
        for j in range(D // HB):
            v = tok[rows, j * HB : (j + 1) * HB].astype(F32)
            total = total + v * v
        scale_col[rows, :] = total
        return carry

    def own_step(i, carry):
        rows = pl.ds(pl.multiple_of(i * 64, 64), 64)
        s = lax.rsqrt(jnp.sum(scale_col[rows, :], axis=1, keepdims=True) * (1.0 / D) + norm_eps)
        scale_col[rows, :] = jnp.broadcast_to(s, (64, HB))
        own[rows, :] = (tok[rows, cols(c, COL)].astype(F32) * s).astype(BF16)
        return carry

    for n in range(4):
        tok_loads[n].wait()
        with jax.named_scope("square"):
            lax.fori_loop(n * 8, n * 8 + 8, square_step, 0, unroll=2)
    weight_loads = [load(7, gate_in, gate_f), load(8, up_in, up_f), load(9, dn_in, dn_f)]
    for copy in shared_loads:
        copy.wait()
    shgu[block(f, 256), 0:HB] = (shg_f[...] * gain_col[...]).astype(BF16)
    shgu[block(f, 256), HB : 2 * HB] = (shu_f[...] * gain_col[...]).astype(BF16)
    sdcol[block(f, 64), :] = shd_f[...].astype(BF16)
    with jax.named_scope("barrier"):
        pl.semaphore_wait(barrier, 22)
    spread_first("sh", shgu, 256)
    with jax.named_scope("own"):
        lax.fori_loop(0, TOK // 64, own_step, 0)

    def token_first(n):
        start, height = CHUNKS[n]
        for s in range(start // CAP, (start + height) // CAP):
            if s:
                arrive(arrived.at[pl.ds(s * CAP, CAP), cols(c, COL)], ("tok", s))
        piece = arrived.at[pl.ds(start, height), cols(c, COL)]
        send(piece, piece, ("xm", n), tp_dev(1))
        send(piece, piece, ("xp", n), tp_dev(3))
        send(piece, piece, ("kp", n, 0), partner)

    def token_second(n):
        start, height = CHUNKS[n]
        half = height // 2
        for name, d, then, on, skip in (("xm", 3, "ft", 1, 0), ("xp", 1, "fb", 3, half)):
            piece = arrived.at[pl.ds(start, height), cols(tp_of(d), COL)]
            arrive(piece, (name, n))
            part = arrived.at[pl.ds(start + skip, half), cols(tp_of(d), COL)]
            send(part, part, (then, n), tp_dev(on))
            send(piece, piece, ("kp", n, d), partner)

    def token_third(n):
        start, height = CHUNKS[n]
        half = height // 2
        for name, skip in (("ft", 0), ("fb", half)):
            part = arrived.at[pl.ds(start + skip, half), cols(tp_of(2), COL)]
            arrive(part, (name, n))
        piece = arrived.at[pl.ds(start, height), cols(tp_of(2), COL)]
        send(piece, piece, ("kp", n, 2), partner)

    def token_last(n):
        start, height = CHUNKS[n]
        for d in range(4):
            arrive(arrived.at[pl.ds(start, height), cols(tp_of(d, 1), COL)], ("kp", n, d))

    with jax.named_scope("dispatch"):
        for g in ORDER:
            s_row = (lax.broadcasted_iota(jnp.int32, (GROUP, TOK), 0) + g * GROUP).astype(F32)
            placing = jnp.where((s_row == t0) | (s_row == t1), 1.0, 0.0).astype(BF16)
            outgoing[g * GROUP : (g + 1) * GROUP, :] = dot(placing, own[...]).astype(BF16)
            for dy in ORDER:
                if (g, dy) != (0, 0):
                    there = ((4 - g) % 4) * 4 + (4 - dy) % 4
                    send(
                        outgoing.at[pl.ds((g * 4 + dy) * CAP, CAP)],
                        arrived.at[pl.ds(there * CAP, CAP), cols(c, COL)],
                        ("tok", there),
                        fs_dev(g, dy),
                    )
            if g == 0:
                arrived[0:CAP, cols(c, COL)] = outgoing[0:CAP, :]
    def gu_step(e, carry):
        gu_send[e, :, 0:HB] = (gate_f[e] * gain_col[...]).astype(BF16)
        gu_send[e, :, HB : 2 * HB] = (up_f[e] * gain_col[...]).astype(BF16)
        return carry

    def gu_first():
        weight_loads[0].wait()
        weight_loads[1].wait()
        lax.fori_loop(0, 16, gu_step, 0)
        gu[block(f, 256), :] = gu_send[f]
        gu_part(0)

    def gu_part(part):
        for oz, oy in FAR:
            there = ((4 - oz) % 4) * 4 + (4 - oy) % 4
            send(
                gu_send.at[fs_of(oz, oy), pl.ds(part * 128, 128)],
                gu.at[pl.ds(pl.multiple_of(f * 256 + part * 128, 128), 128)],
                ("gu", part, there),
                fs_dev(oz, oy),
            )

    def dn_step(e, carry):
        dn_send[e] = dn_f[e].astype(BF16)
        return carry

    def dn_first():
        weight_loads[2].wait()
        lax.fori_loop(0, 16, dn_step, 0)
        for oz, oy in FAR:
            there = ((4 - oz) % 4) * 4 + (4 - oy) % 4
            send(dn_send.at[fs_of(oz, oy)], dcol.at[block(f, 64)], ("dn", there), fs_dev(oz, oy))
        dcol[block(f, 64), :] = dn_send[f]

    def silu_times(gate, up):
        return (gate / (1.0 + jnp.exp(-gate)) * up).astype(BF16)

    def hidden_rows(g):
        return (g * GROUP, GROUP) if g < 4 else (ROWS, TOK)

    def hidden_first(g):
        start, height = hidden_rows(g)
        piece = hid.at[pl.ds(start, height), cols(c, HB)]
        send(piece, piece, ("hm", g), tp_dev(1))
        send(piece, piece, ("hp", g), tp_dev(3))
        send(piece, piece, ("hk", g, 0), partner)

    def hidden_second(g):
        start, height = hidden_rows(g)
        half = height // 2
        for name, d, then, on, skip in (("hm", 3, "ht", 1, 0), ("hp", 1, "hb", 3, half)):
            piece = hid.at[pl.ds(start, height), cols(tp_of(d), HB)]
            arrive(piece, (name, g))
            part = hid.at[pl.ds(start + skip, half), cols(tp_of(d), HB)]
            send(part, part, (then, g), tp_dev(on))
            send(piece, piece, ("hk", g, d), partner)

    def hidden_third(g):
        start, height = hidden_rows(g)
        half = height // 2
        for name, skip in (("ht", 0), ("hb", half)):
            part = hid.at[pl.ds(start + skip, half), cols(tp_of(2), HB)]
            arrive(part, (name, g))
        piece = hid.at[pl.ds(start, height), cols(tp_of(2), HB)]
        send(piece, piece, ("hk", g, 2), partner)

    def hidden_last(g):
        start, height = hidden_rows(g)
        for d in range(4):
            arrive(hid.at[pl.ds(start, height), cols(tp_of(d, 1), HB)], ("hk", g, d))

    def expert_hidden(g):
        for n in ((0, 1), (2,), (4,), (3,))[g]:
            token_last(n)
        rows = pl.ds(g * GROUP, GROUP)
        both = dot(arrived[rows, :], gu[...])
        hid[rows, cols(c, HB)] = silu_times(both[:, 0:HB], both[:, HB:])
        hidden_first(g)

    def expert_down(g):
        hidden_last(g)
        rows = pl.ds(g * GROUP, GROUP)
        rsend[rows, :] = dot(hid[rows, :], dcol[...]).astype(BF16)
        for dy in ORDER:
            if (g, dy) != (0, 0):
                there = ((4 - g) % 4) * 4 + (4 - dy) % 4
                send(
                    rsend.at[pl.ds((g * 4 + dy) * CAP, CAP)],
                    ret.at[pl.ds(there * CAP, CAP)],
                    ("ret", there),
                    fs_dev(g, dy),
                )
        if g == 0:
            ret[0:CAP, :] = rsend[0:CAP, :]

    def across(name, src, dst, some):
        for d in some:
            for other in range(2):
                if (d, other) != (0, 0):
                    send(
                        src.at[cols(tp_of(d, other), HB)],
                        dst.at[:, cols(c, COL)],
                        (name, (4 - d) % 4, other),
                        tp_dev(d, other),
                    )
        if 0 in some:
            dst[:, cols(c, COL)] = src[cols(c, HB), :]

    def across_last(name, dst):
        for d in range(4):
            for other in range(2):
                if (d, other) != (0, 0):
                    arrive(dst.at[:, cols(tp_of(d, other), COL)], (name, d, other))

    def norm_step(i, carry):
        rows = pl.ds(pl.multiple_of(i * 16, 16), 16)
        tok[rows, :] = (tok[rows, :].astype(F32) * scale_col[rows, 0:1]).astype(BF16)
        return carry

    def combine_weights():
        packed = jnp.concatenate([t0, t1, weight[...], jnp.zeros((4, TOK), F32)], axis=0)
        by_token = packed.T
        for g in range(4):
            s_col = (lax.broadcasted_iota(jnp.int32, (TOK, GROUP), 1) + g * GROUP).astype(F32)
            comb[:, g * GROUP : (g + 1) * GROUP] = (
                jnp.where(s_col == by_token[:, 0:1], by_token[:, 2:3], 0.0)
                + jnp.where(s_col == by_token[:, 1:2], by_token[:, 3:4], 0.0)
            ).astype(BF16)

    def gu_last():
        for part in range(2):
            for oz, oy in NEAR:
                start = pl.multiple_of(fs_of(oz, oy) * 256 + part * 128, 128)
                arrive(gu.at[pl.ds(start, 128)], ("gu", part, oz * 4 + oy))

    def dn_last():
        for oz, oy in NEAR:
            arrive(dcol.at[block(fs_of(oz, oy), 64)], ("dn", oz * 4 + oy))

    def shared_hidden():
        spread_last("sh", shgu, 256)
        acc[...] = jnp.zeros((TOK, 2 * HB), F32)

        def step(i, carry):
            acc[...] += dot(tok[:, block(i, COL)], shgu[block(i, COL), :])
            return carry

        lax.fori_loop(0, 8, step, 0)
        hid[ROWS : ROWS + TOK, cols(c, HB)] = silu_times(acc[:, 0:HB], acc[:, HB:])
        hidden_first(4)

    def shared_down():
        hidden_last(4)
        macc[...] = dot(hid[ROWS : ROWS + TOK, :], sdcol[...])

    def combine(g):
        oz = (4 - g) % 4
        for oy in ORDER:
            if (oz, oy) != (0, 0):
                s = oz * 4 + oy
                arrive(ret.at[pl.ds(s * CAP, CAP)], ("ret", s))
        macc[...] += dot(comb[:, oz * GROUP : (oz + 1) * GROUP], ret[oz * GROUP : (oz + 1) * GROUP])

    steps = dict(
        t1=token_first,
        t2=token_second,
        t3=token_third,
        eh=expert_hidden,
        h2=hidden_second,
        h3=hidden_third,
        ed=expert_down,
        cb=combine,
    )
    singles = dict(
        norm=lambda: lax.fori_loop(0, TOK // 16, norm_step, 0, unroll=2),
        comb=combine_weights,
        gu=gu_last,
        dn=dn_last,
        gu1=gu_first,
        gu2=lambda: gu_part(1),
        dn1=dn_first,
        sh1=lambda: spread_first("sh", shgu, 256),
        sh2=lambda: spread_second("sh", shgu, 256),
        sd1=lambda: spread_first("sd", sdcol, 64),
        sd2=lambda: spread_second("sd", sdcol, 64),
        sd3=lambda: spread_last("sd", sdcol, 64),
        sh=shared_hidden,
        sdn=shared_down,
        dxa=lambda: across("dx", dcol, drow, (2, 0)),
        dxb=lambda: across("dx", dcol, drow, (1, 3)),
        sxa=lambda: across("sx", sdcol, sdrow, (2, 0)),
        sxb=lambda: across("sx", sdcol, sdrow, (1, 3)),
        dx3=lambda: across_last("dx", drow),
        sx3=lambda: across_last("sx", sdrow),
    )
    for word in PLAN:
        with jax.named_scope(word.replace(":", "_")):
            if ":" in word:
                name, n = word.split(":")
                steps[name](int(n))
            else:
                singles[word]()
    mixv[...] = macc[...].astype(BF16)
    with jax.named_scope("drain"):
        for copy in sent:
            copy.wait_send()


def writer(gu, drow, shgu, sdrow, mixv, eg, eu, ed, sg, su, sd, mix, sems):
    copies = [
        pltpu.make_async_copy(src, dst, sems.at[n])
        for n, (src, dst) in enumerate(
            (
                (gu.at[:, pl.ds(0, HB)], eg.at[0]),
                (gu.at[:, pl.ds(HB, HB)], eu.at[0]),
                (drow, ed.at[0]),
                (shgu.at[:, pl.ds(0, HB)], sg),
                (shgu.at[:, pl.ds(HB, HB)], su),
                (sdrow, sd),
                (mixv, mix),
            )
        )
    ]
    for copy in copies:
        copy.start()
    for copy in copies:
        copy.wait()


def on_device(
    tokens,
    norm_gain,
    gate_train,
    up_train,
    down_train,
    shared_gate_train,
    shared_up_train,
    shared_down_train,
    route_expert,
    route_weight,
):
    hbm = pl.BlockSpec(memory_space=pl.ANY)
    vmem = pl.BlockSpec(memory_space=pltpu.VMEM)
    kept = pl.pallas_call(
        kernel,
        out_shape=(
            pltpu.VMEM((D, 2 * HB), BF16),
            pltpu.VMEM((HB, D), BF16),
            pltpu.VMEM((D, 2 * HB), BF16),
            pltpu.VMEM((HB, D), BF16),
            pltpu.VMEM((TOK, COL), BF16),
        ),
        in_specs=[hbm, vmem, hbm, hbm, hbm, hbm, hbm, hbm, vmem, vmem],
        out_specs=(vmem,) * 5,
        scratch_shapes=[
            pltpu.VMEM((TOK, D), BF16),
            pltpu.VMEM((16, 256, HB), F32),
            pltpu.VMEM((16, 256, HB), F32),
            pltpu.VMEM((16, 64, COL), F32),
            pltpu.VMEM((256, HB), F32),
            pltpu.VMEM((256, HB), F32),
            pltpu.VMEM((64, COL), F32),
            pltpu.VMEM((256, HB), F32),
            pltpu.VMEM((TOK, HB), F32),
            pltpu.VMEM((TOK, COL), BF16),
            pltpu.VMEM((ROWS, COL), BF16),
            pltpu.VMEM((ROWS, D), BF16),
            pltpu.VMEM((16, 256, 2 * HB), BF16),
            pltpu.VMEM((16, 64, COL), BF16),
            pltpu.VMEM((H, COL), BF16),
            pltpu.VMEM((H, COL), BF16),
            pltpu.VMEM((TOK, 2 * HB), F32),
            pltpu.VMEM((ROWS + TOK, H), BF16),
            pltpu.VMEM((ROWS, COL), BF16),
            pltpu.VMEM((ROWS, COL), BF16),
            pltpu.VMEM((TOK, ROWS), BF16),
            pltpu.VMEM((TOK, COL), F32),
            pltpu.SemaphoreType.DMA((224,)),
            pltpu.SemaphoreType.DMA((224,)),
            pltpu.SemaphoreType.DMA((10,)),
        ],
        compiler_params=pltpu.CompilerParams(
            collective_id=0, has_side_effects=True, vmem_limit_bytes=54 * 1024 * 1024
        ),
        name="layer",
    )(
        tokens,
        norm_gain.reshape(1, 256),
        gate_train,
        up_train,
        down_train,
        shared_gate_train,
        shared_up_train,
        shared_down_train,
        route_expert.T,
        route_weight.T,
    )
    return pl.pallas_call(
        writer,
        out_shape=(
            jax.ShapeDtypeStruct((1, D, HB), BF16),
            jax.ShapeDtypeStruct((1, D, HB), BF16),
            jax.ShapeDtypeStruct((1, HB, D), BF16),
            jax.ShapeDtypeStruct((D, HB), BF16),
            jax.ShapeDtypeStruct((D, HB), BF16),
            jax.ShapeDtypeStruct((HB, D), BF16),
            jax.ShapeDtypeStruct((TOK, COL), BF16),
        ),
        in_specs=[vmem] * 5,
        out_specs=(hbm,) * 7,
        scratch_shapes=[pltpu.SemaphoreType.DMA((7,))],
        compiler_params=pltpu.CompilerParams(vmem_limit_bytes=1024 * 1024),
        name="writer",
    )(*(pltpu.with_memory_space_constraint(a, pltpu.VMEM) for a in kept))


def solution(mesh):
    placed = (
        P("fs", None),
        P("fs"),
        P(None, "fs", "tp"),
        P(None, "fs", "tp"),
        P(None, "fs", "tp"),
        P("fs", "tp"),
        P("fs", "tp"),
        P("fs", "tp"),
        P("fs", None),
        P("fs", None),
    )
    return jax.shard_map(
        on_device,
        mesh=mesh,
        in_specs=placed,
        out_specs=(
            P("fs", None, "tp"),
            P("fs", None, "tp"),
            P("fs", "tp", None),
            P(None, "tp"),
            P(None, "tp"),
            P("tp", None),
            P("fs", "tp"),
        ),
        check_vma=False,
    )
```

```python
import jax
import jax.numpy as jnp
from jax import lax
from jax.experimental import pallas as pl
from jax.experimental.pallas import tpu as pltpu
from jax.sharding import PartitionSpec as P

norm_eps = 1e-06
MESH = pl.DeviceIdType.MESH
F32 = jnp.float32
BF16 = jnp.bfloat16
CAP = 96
GROUP = 4 * CAP
HALF = GROUP // 2
TOK = 512
D = 4096
COL = 512
H = 1024
HB = 128
ROWS = 16 * CAP
ORDER = (0, 1, 3, 2)
NEAR = [(a, b) for a in ORDER for b in ORDER if (a, b) != (0, 0)]
FAR = NEAR[::-1]
CHUNKS = ((0, CAP), (CAP, 3 * CAP), (GROUP, GROUP), (3 * GROUP, GROUP), (2 * GROUP, GROUP))

PLAN = (
    "t1:0", "sd1", "gu1", "gu2", "sh2", "dn1", "t1:1", "t2:0", "comb", "norm", "t1:2", "t2:1",
    "t3:0", "t1:3", "t1:4", "t2:2", "t3:1", "t2:3", "t3:2", "sd2", "t2:4", "t3:3", "gu", "eh:0",
    "eh:1", "t3:4", "eh:3", "h2:0", "eh:2", "h2:1", "sh", "h3:0", "h2:3", "h3:1", "h2:2",
    "h2:4", "dn", "dxa", "dxb", "ed:0", "ed:1", "h3:3", "h3:2", "ed:3", "h3:4", "ed:2", "sd3",
    "sxa", "sxb", "sdn", "cb:0", "cb:1", "cb:3", "cb:2", "dx3", "sx3",
)


def dot(a, b):
    return jnp.dot(a, b, preferred_element_type=F32)


def kernel(
    tok_in,
    gain_in,
    gate_in,
    up_in,
    dn_in,
    shg_in,
    shu_in,
    shd_in,
    route,
    weight,
    gu,
    drow,
    shgu,
    sdrow,
    mixv,
    tok,
    gate_f,
    up_f,
    dn_f,
    shg_f,
    shu_f,
    shd_f,
    gain_col,
    scale_col,
    own,
    outgoing,
    arrived,
    gu_send,
    dn_send,
    dcol,
    sdcol,
    acc,
    hid,
    rsend,
    ret,
    comb,
    macc,
    ss,
    rs,
    ls,
):
    f = lax.axis_index("fs")
    c = lax.axis_index("tp")
    z, y = f // 4, f % 4
    x, k = c // 2, c % 2

    def fs_of(oz, oy):
        return ((z + oz) % 4) * 4 + (y + oy) % 4

    def tp_of(d, other=0):
        return ((x + d) % 4) * 2 + (k + other) % 2

    def fs_dev(oz, oy):
        return (fs_of(oz, oy), c)

    def tp_dev(d, other=0):
        return (f, tp_of(d, other))

    partner = tp_dev(0, 1)
    sent = []
    keys = {}

    def place(key):
        return keys.setdefault(key, len(keys))

    def send(src, dst, key, dev):
        copy = pltpu.make_async_remote_copy(
            src_ref=src,
            dst_ref=dst,
            send_sem=ss.at[len(sent)],
            recv_sem=rs.at[place(key)],
            device_id=dev,
            device_id_type=MESH,
        )
        copy.start()
        sent.append(copy)

    def arrive(dst, key):
        pltpu.make_async_remote_copy(
            src_ref=dst,
            dst_ref=dst,
            send_sem=ss.at[0],
            recv_sem=rs.at[place(key)],
            device_id=partner,
            device_id_type=MESH,
        ).wait_recv()

    def cols(tp_index, width):
        return pl.ds(pl.multiple_of(tp_index * width, width), width)

    def block(index, width):
        return pl.ds(pl.multiple_of(index * width, width), width)

    def load(n, src, dst):
        copy = pltpu.make_async_copy(src, dst, ls.at[n])
        copy.start()
        return copy

    quarter = TOK // 4
    tok_loads = [
        load(n, tok_in.at[pl.ds(n * quarter, quarter)], tok.at[pl.ds(n * quarter, quarter)])
        for n in range(4)
    ]
    shared_loads = [load(4, shg_in, shg_f), load(5, shu_in, shu_f), load(6, shd_in, shd_f)]

    barrier = pltpu.get_barrier_semaphore()
    for oz, oy in NEAR:
        pl.semaphore_signal(barrier, inc=1, device_id=fs_dev(oz, oy), device_id_type=MESH)
    for d in range(4):
        for other in range(2):
            if (d, other) != (0, 0):
                pl.semaphore_signal(
                    barrier, inc=1, device_id=tp_dev(d, other), device_id_type=MESH
                )

    def line(j, d):
        return fs_of(k * j + (1 - k) * d, (1 - k) * j + k * d)

    def spread_first(name, ref, height):
        piece = ref.at[block(f, height)]
        for d in (2, 1, 3):
            send(piece, piece, (name, 4 - d), (line(d, 0), c))

    def spread_second(name, ref, height):
        for j in (0, 1, 3, 2):
            piece = ref.at[block(line(j, 0), height)]
            if j:
                arrive(piece, (name, j))
            for d in (2, 1, 3):
                send(piece, piece, (name, j, 4 - d), (line(0, d), c))

    def spread_last(name, ref, height):
        for j in range(4):
            for d in (1, 2, 3):
                arrive(ref.at[block(line(j, d), height)], (name, j, d))

    r0, r1 = route[0:1, :], route[1:2, :]
    e_row = lax.broadcasted_iota(jnp.int32, (16, TOK), 0)
    is0, is1 = e_row == r0, e_row == r1
    named = jnp.where(is0 | is1, 1.0, 0.0).astype(BF16)
    before = jnp.where(
        lax.broadcasted_iota(jnp.int32, (TOK, TOK), 0)
        < lax.broadcasted_iota(jnp.int32, (TOK, TOK), 1),
        1.0,
        0.0,
    ).astype(BF16)
    earlier = dot(named, before)

    def target_of(r, hit):
        slot = jnp.sum(jnp.where(hit, earlier, 0.0), axis=0, keepdims=True)
        relative = (((r // 4) - z + 4) % 4) * 4 + ((r % 4) - y + 4) % 4
        return relative.astype(F32) * float(CAP) + slot

    t0, t1 = target_of(r0, is0), target_of(r1, is1)

    diag = lax.broadcasted_iota(jnp.int32, (256, 256), 0) == lax.broadcasted_iota(
        jnp.int32, (256, 256), 1
    )
    gain_col[...] = jnp.broadcast_to(
        jnp.sum(jnp.where(diag, gain_in[...], 0.0), axis=1, keepdims=True), (256, HB)
    )

    def square_step(i, carry):
        rows = pl.ds(pl.multiple_of(i * 16, 16), 16)
        total = jnp.zeros((16, HB), F32)
        for j in range(D // HB):
            v = tok[rows, j * HB : (j + 1) * HB].astype(F32)
            total = total + v * v
        scale_col[rows, :] = total
        return carry

    def own_step(i, carry):
        rows = pl.ds(pl.multiple_of(i * 64, 64), 64)
        s = lax.rsqrt(jnp.sum(scale_col[rows, :], axis=1, keepdims=True) * (1.0 / D) + norm_eps)
        scale_col[rows, :] = jnp.broadcast_to(s, (64, HB))
        own[rows, :] = (tok[rows, cols(c, COL)].astype(F32) * s).astype(BF16)
        return carry

    for n in range(4):
        tok_loads[n].wait()
        with jax.named_scope("square"):
            lax.fori_loop(n * 8, n * 8 + 8, square_step, 0, unroll=4)
    weight_loads = [load(7, gate_in, gate_f), load(8, up_in, up_f), load(9, dn_in, dn_f)]
    for copy in shared_loads:
        copy.wait()
    shgu[block(f, 256), 0:HB] = (shg_f[...] * gain_col[...]).astype(BF16)
    shgu[block(f, 256), HB : 2 * HB] = (shu_f[...] * gain_col[...]).astype(BF16)
    sdcol[block(f, 64), :] = shd_f[...].astype(BF16)
    with jax.named_scope("barrier"):
        pl.semaphore_wait(barrier, 22)
    spread_first("sh", shgu, 256)
    with jax.named_scope("own"):
        lax.fori_loop(0, TOK // 64, own_step, 0, unroll=4)

    def token_first(n):
        start, height = CHUNKS[n]
        for s in range(start // CAP, (start + height) // CAP):
            if s:
                arrive(arrived.at[pl.ds(s * CAP, CAP), cols(c, COL)], ("tok", s))
        piece = arrived.at[pl.ds(start, height), cols(c, COL)]
        send(piece, piece, ("xm", n), tp_dev(1))
        send(piece, piece, ("xp", n), tp_dev(3))
        send(piece, piece, ("kp", n, 0), partner)

    def token_second(n):
        start, height = CHUNKS[n]
        half = height // 2
        for name, d, then, on, skip in (("xm", 3, "ft", 1, 0), ("xp", 1, "fb", 3, half)):
            piece = arrived.at[pl.ds(start, height), cols(tp_of(d), COL)]
            arrive(piece, (name, n))
            part = arrived.at[pl.ds(start + skip, half), cols(tp_of(d), COL)]
            send(part, part, (then, n), tp_dev(on))
            send(piece, piece, ("kp", n, d), partner)

    def token_third(n):
        start, height = CHUNKS[n]
        half = height // 2
        for name, skip in (("ft", 0), ("fb", half)):
            part = arrived.at[pl.ds(start + skip, half), cols(tp_of(2), COL)]
            arrive(part, (name, n))
        piece = arrived.at[pl.ds(start, height), cols(tp_of(2), COL)]
        send(piece, piece, ("kp", n, 2), partner)

    def token_last(n):
        start, height = CHUNKS[n]
        for d in range(4):
            arrive(arrived.at[pl.ds(start, height), cols(tp_of(d, 1), COL)], ("kp", n, d))

    with jax.named_scope("dispatch"):
        for g in ORDER:
            s_row = (lax.broadcasted_iota(jnp.int32, (GROUP, TOK), 0) + g * GROUP).astype(F32)
            placing = jnp.where((s_row == t0) | (s_row == t1), 1.0, 0.0).astype(BF16)
            outgoing[g * GROUP : (g + 1) * GROUP, :] = dot(placing, own[...]).astype(BF16)
            for dy in ORDER:
                if (g, dy) != (0, 0):
                    there = ((4 - g) % 4) * 4 + (4 - dy) % 4
                    send(
                        outgoing.at[pl.ds((g * 4 + dy) * CAP, CAP)],
                        arrived.at[pl.ds(there * CAP, CAP), cols(c, COL)],
                        ("tok", there),
                        fs_dev(g, dy),
                    )
            if g == 0:
                arrived[0:CAP, cols(c, COL)] = outgoing[0:CAP, :]
    def gu_step(e, carry):
        gu_send[e, :, 0:HB] = (gate_f[e] * gain_col[...]).astype(BF16)
        gu_send[e, :, HB : 2 * HB] = (up_f[e] * gain_col[...]).astype(BF16)
        return carry

    def gu_first():
        weight_loads[0].wait()
        weight_loads[1].wait()
        lax.fori_loop(0, 16, gu_step, 0)
        gu[block(f, 256), :] = gu_send[f]
        gu_part(0)

    def gu_part(part):
        for oz, oy in FAR:
            there = ((4 - oz) % 4) * 4 + (4 - oy) % 4
            send(
                gu_send.at[fs_of(oz, oy), pl.ds(part * 128, 128)],
                gu.at[pl.ds(pl.multiple_of(f * 256 + part * 128, 128), 128)],
                ("gu", part, there),
                fs_dev(oz, oy),
            )

    def dn_step(e, carry):
        dn_send[e] = dn_f[e].astype(BF16)
        return carry

    def dn_first():
        weight_loads[2].wait()
        lax.fori_loop(0, 16, dn_step, 0)
        for oz, oy in FAR:
            there = ((4 - oz) % 4) * 4 + (4 - oy) % 4
            send(dn_send.at[fs_of(oz, oy)], dcol.at[block(f, 64)], ("dn", there), fs_dev(oz, oy))
        dcol[block(f, 64), :] = dn_send[f]

    def silu_times(gate, up):
        return (gate / (1.0 + jnp.exp(-gate)) * up).astype(BF16)

    def hidden_rows(g):
        return (g * GROUP, GROUP) if g < 4 else (ROWS, TOK)

    def hidden_first(g):
        start, height = hidden_rows(g)
        piece = hid.at[pl.ds(start, height), cols(c, HB)]
        send(piece, piece, ("hm", g), tp_dev(1))
        send(piece, piece, ("hp", g), tp_dev(3))
        send(piece, piece, ("hk", g, 0), partner)

    def hidden_second(g):
        start, height = hidden_rows(g)
        half = height // 2
        for name, d, then, on, skip in (("hm", 3, "ht", 1, 0), ("hp", 1, "hb", 3, half)):
            piece = hid.at[pl.ds(start, height), cols(tp_of(d), HB)]
            arrive(piece, (name, g))
            part = hid.at[pl.ds(start + skip, half), cols(tp_of(d), HB)]
            send(part, part, (then, g), tp_dev(on))
            send(piece, piece, ("hk", g, d), partner)

    def hidden_third(g):
        start, height = hidden_rows(g)
        half = height // 2
        for name, skip in (("ht", 0), ("hb", half)):
            part = hid.at[pl.ds(start + skip, half), cols(tp_of(2), HB)]
            arrive(part, (name, g))
        piece = hid.at[pl.ds(start, height), cols(tp_of(2), HB)]
        send(piece, piece, ("hk", g, 2), partner)

    def hidden_last(g):
        start, height = hidden_rows(g)
        for d in range(4):
            arrive(hid.at[pl.ds(start, height), cols(tp_of(d, 1), HB)], ("hk", g, d))

    def expert_hidden(g):
        for n in ((0, 1), (2,), (4,), (3,))[g]:
            token_last(n)
        rows = pl.ds(g * GROUP, GROUP)
        both = dot(arrived[rows, :], gu[...])
        hid[rows, cols(c, HB)] = silu_times(both[:, 0:HB], both[:, HB:])
        hidden_first(g)

    def expert_down(g):
        hidden_last(g)
        rows = pl.ds(g * GROUP, GROUP)
        rsend[rows, :] = dot(hid[rows, :], dcol[...]).astype(BF16)
        for dy in ORDER:
            if (g, dy) != (0, 0):
                there = ((4 - g) % 4) * 4 + (4 - dy) % 4
                send(
                    rsend.at[pl.ds((g * 4 + dy) * CAP, CAP)],
                    ret.at[pl.ds(there * CAP, CAP)],
                    ("ret", there),
                    fs_dev(g, dy),
                )
        if g == 0:
            ret[0:CAP, :] = rsend[0:CAP, :]

    def across(name, src, dst, some):
        for d in some:
            for other in range(2):
                if (d, other) != (0, 0):
                    send(
                        src.at[cols(tp_of(d, other), HB)],
                        dst.at[:, cols(c, COL)],
                        (name, (4 - d) % 4, other),
                        tp_dev(d, other),
                    )
        if 0 in some:
            dst[:, cols(c, COL)] = src[cols(c, HB), :]

    def across_last(name, dst):
        for d in range(4):
            for other in range(2):
                if (d, other) != (0, 0):
                    arrive(dst.at[:, cols(tp_of(d, other), COL)], (name, d, other))

    def norm_step(i, carry):
        rows = pl.ds(pl.multiple_of(i * 16, 16), 16)
        tok[rows, :] = (tok[rows, :].astype(F32) * scale_col[rows, 0:1]).astype(BF16)
        return carry

    def combine_weights():
        packed = jnp.concatenate([t0, t1, weight[...], jnp.zeros((4, TOK), F32)], axis=0)
        by_token = packed.T
        for g in range(4):
            s_col = (lax.broadcasted_iota(jnp.int32, (TOK, GROUP), 1) + g * GROUP).astype(F32)
            comb[:, g * GROUP : (g + 1) * GROUP] = (
                jnp.where(s_col == by_token[:, 0:1], by_token[:, 2:3], 0.0)
                + jnp.where(s_col == by_token[:, 1:2], by_token[:, 3:4], 0.0)
            ).astype(BF16)

    def gu_last():
        for part in range(2):
            for oz, oy in NEAR:
                start = pl.multiple_of(fs_of(oz, oy) * 256 + part * 128, 128)
                arrive(gu.at[pl.ds(start, 128)], ("gu", part, oz * 4 + oy))

    def dn_last():
        for oz, oy in NEAR:
            arrive(dcol.at[block(fs_of(oz, oy), 64)], ("dn", oz * 4 + oy))

    def shared_hidden():
        spread_last("sh", shgu, 256)
        acc[...] = jnp.zeros((TOK, 2 * HB), F32)

        def step(i, carry):
            acc[...] += dot(tok[:, block(i, COL)], shgu[block(i, COL), :])
            return carry

        lax.fori_loop(0, 8, step, 0)
        hid[ROWS : ROWS + TOK, cols(c, HB)] = silu_times(acc[:, 0:HB], acc[:, HB:])
        hidden_first(4)

    def shared_down():
        hidden_last(4)
        macc[...] = dot(hid[ROWS : ROWS + TOK, :], sdcol[...])

    def combine(g):
        oz = (4 - g) % 4
        for oy in ORDER:
            if (oz, oy) != (0, 0):
                s = oz * 4 + oy
                arrive(ret.at[pl.ds(s * CAP, CAP)], ("ret", s))
        macc[...] += dot(comb[:, oz * GROUP : (oz + 1) * GROUP], ret[oz * GROUP : (oz + 1) * GROUP])

    steps = dict(
        t1=token_first,
        t2=token_second,
        t3=token_third,
        eh=expert_hidden,
        h2=hidden_second,
        h3=hidden_third,
        ed=expert_down,
        cb=combine,
    )
    singles = dict(
        norm=lambda: lax.fori_loop(0, TOK // 16, norm_step, 0, unroll=2),
        comb=combine_weights,
        gu=gu_last,
        dn=dn_last,
        gu1=gu_first,
        gu2=lambda: gu_part(1),
        dn1=dn_first,
        sh1=lambda: spread_first("sh", shgu, 256),
        sh2=lambda: spread_second("sh", shgu, 256),
        sd1=lambda: spread_first("sd", sdcol, 64),
        sd2=lambda: spread_second("sd", sdcol, 64),
        sd3=lambda: spread_last("sd", sdcol, 64),
        sh=shared_hidden,
        sdn=shared_down,
        dxa=lambda: across("dx", dcol, drow, (2, 0)),
        dxb=lambda: across("dx", dcol, drow, (1, 3)),
        sxa=lambda: across("sx", sdcol, sdrow, (2, 0)),
        sxb=lambda: across("sx", sdcol, sdrow, (1, 3)),
        dx3=lambda: across_last("dx", drow),
        sx3=lambda: across_last("sx", sdrow),
    )
    for word in PLAN:
        with jax.named_scope(word.replace(":", "_")):
            if ":" in word:
                name, n = word.split(":")
                steps[name](int(n))
            else:
                singles[word]()
    mixv[...] = macc[...].astype(BF16)
    with jax.named_scope("drain"):
        for copy in sent:
            copy.wait_send()


def writer(gu, drow, shgu, sdrow, mixv, eg, eu, ed, sg, su, sd, mix, sems):
    copies = [
        pltpu.make_async_copy(src, dst, sems.at[n])
        for n, (src, dst) in enumerate(
            (
                (gu.at[:, pl.ds(0, HB)], eg.at[0]),
                (gu.at[:, pl.ds(HB, HB)], eu.at[0]),
                (drow, ed.at[0]),
                (shgu.at[:, pl.ds(0, HB)], sg),
                (shgu.at[:, pl.ds(HB, HB)], su),
                (sdrow, sd),
                (mixv, mix),
            )
        )
    ]
    for copy in copies:
        copy.start()
    for copy in copies:
        copy.wait()


def on_device(
    tokens,
    norm_gain,
    gate_train,
    up_train,
    down_train,
    shared_gate_train,
    shared_up_train,
    shared_down_train,
    route_expert,
    route_weight,
):
    hbm = pl.BlockSpec(memory_space=pl.ANY)
    vmem = pl.BlockSpec(memory_space=pltpu.VMEM)
    kept = pl.pallas_call(
        kernel,
        out_shape=(
            pltpu.VMEM((D, 2 * HB), BF16),
            pltpu.VMEM((HB, D), BF16),
            pltpu.VMEM((D, 2 * HB), BF16),
            pltpu.VMEM((HB, D), BF16),
            pltpu.VMEM((TOK, COL), BF16),
        ),
        in_specs=[hbm, vmem, hbm, hbm, hbm, hbm, hbm, hbm, vmem, vmem],
        out_specs=(vmem,) * 5,
        scratch_shapes=[
            pltpu.VMEM((TOK, D), BF16),
            pltpu.VMEM((16, 256, HB), F32),
            pltpu.VMEM((16, 256, HB), F32),
            pltpu.VMEM((16, 64, COL), F32),
            pltpu.VMEM((256, HB), F32),
            pltpu.VMEM((256, HB), F32),
            pltpu.VMEM((64, COL), F32),
            pltpu.VMEM((256, HB), F32),
            pltpu.VMEM((TOK, HB), F32),
            pltpu.VMEM((TOK, COL), BF16),
            pltpu.VMEM((ROWS, COL), BF16),
            pltpu.VMEM((ROWS, D), BF16),
            pltpu.VMEM((16, 256, 2 * HB), BF16),
            pltpu.VMEM((16, 64, COL), BF16),
            pltpu.VMEM((H, COL), BF16),
            pltpu.VMEM((H, COL), BF16),
            pltpu.VMEM((TOK, 2 * HB), F32),
            pltpu.VMEM((ROWS + TOK, H), BF16),
            pltpu.VMEM((ROWS, COL), BF16),
            pltpu.VMEM((ROWS, COL), BF16),
            pltpu.VMEM((TOK, ROWS), BF16),
            pltpu.VMEM((TOK, COL), F32),
            pltpu.SemaphoreType.DMA((224,)),
            pltpu.SemaphoreType.DMA((224,)),
            pltpu.SemaphoreType.DMA((10,)),
        ],
        compiler_params=pltpu.CompilerParams(
            collective_id=0, has_side_effects=True, vmem_limit_bytes=54 * 1024 * 1024
        ),
        name="layer",
    )(
        tokens,
        norm_gain.reshape(1, 256),
        gate_train,
        up_train,
        down_train,
        shared_gate_train,
        shared_up_train,
        shared_down_train,
        route_expert.T,
        route_weight.T,
    )
    return pl.pallas_call(
        writer,
        out_shape=(
            jax.ShapeDtypeStruct((1, D, HB), BF16),
            jax.ShapeDtypeStruct((1, D, HB), BF16),
            jax.ShapeDtypeStruct((1, HB, D), BF16),
            jax.ShapeDtypeStruct((D, HB), BF16),
            jax.ShapeDtypeStruct((D, HB), BF16),
            jax.ShapeDtypeStruct((HB, D), BF16),
            jax.ShapeDtypeStruct((TOK, COL), BF16),
        ),
        in_specs=[vmem] * 5,
        out_specs=(hbm,) * 7,
        scratch_shapes=[pltpu.SemaphoreType.DMA((7,))],
        compiler_params=pltpu.CompilerParams(vmem_limit_bytes=1024 * 1024),
        name="writer",
    )(*(pltpu.with_memory_space_constraint(a, pltpu.VMEM) for a in kept))


def solution(mesh):
    placed = (
        P("fs", None),
        P("fs"),
        P(None, "fs", "tp"),
        P(None, "fs", "tp"),
        P(None, "fs", "tp"),
        P("fs", "tp"),
        P("fs", "tp"),
        P("fs", "tp"),
        P("fs", None),
        P("fs", None),
    )
    return jax.shard_map(
        on_device,
        mesh=mesh,
        in_specs=placed,
        out_specs=(
            P("fs", None, "tp"),
            P("fs", None, "tp"),
            P("fs", "tp", None),
            P(None, "tp"),
            P(None, "tp"),
            P("tp", None),
            P("fs", "tp"),
        ),
        check_vma=False,
    )
```
